128 devices in a mesh: sp: 16 (over z, y), tp: 8 (over x, core).
Axes of the slice: x: 4, y: 4, z: 4, core: 2. Of those that a mesh axis runs over, the one named last changes fastest.
Arguments:
- resid: bfloat16 [24576, 2048], P(('sp', 'tp')), may hold values from -6 to 6
- cond: bfloat16 [2048], P('sp'), may hold values from -6 to 6
- mod_shift: bfloat16 [2048, 2048], P('sp', 'tp'), may hold values from -0.125 to 0.125
- mod_scale: bfloat16 [2048, 2048], P('sp', 'tp'), may hold values from -0.125 to 0.125
- mod_gate: bfloat16 [2048, 2048], P('sp', 'tp'), may hold values from -0.125 to 0.125
- norm_gain: float32 [2048], replicated, may hold values from 0.1 to 1.9
- context: bfloat16 [1024, 2048], P('sp'), may hold values from -6 to 6
- w_query: bfloat16 [2048, 2048], P(None, 'tp'), may hold values from -0.125 to 0.125
- w_key: bfloat16 [2048, 2048], P(None, 'tp'), may hold values from -0.125 to 0.125
- w_value: bfloat16 [2048, 2048], P(None, 'tp'), may hold values from -0.125 to 0.125
- query_gain: float32 [128], replicated, may hold values from 0.5 to 6, as said below
- key_gain: float32 [128], replicated, may hold values from 0.5 to 6, as said below
- offset_bias: float32 [16, 15, 31], P('tp'), may hold values from -4 to 4
- context_bias: float32 [16], P('tp'), may hold values from -4.5 to 1
- w_out: bfloat16 [2048, 2048], replicated, may hold values from -0.5 to 0.5
Outputs:
- mixed: bfloat16 [24576, 2048], P(('sp', 'tp'))
The draws below stay inside these ranges and needn't reach their ends.
Inputs may be any that keep to these rules, and one draw needn't show every extreme that they name: `query_gain`: positive gains. `key_gain`: positive gains.
All inputs are finite; a program needn't handle non-finite values.
Results may differ from the reference program's by a relative error of at most 0.0085.
The reference program's roundings to bfloat16 on the way count: a program that leaves them out, or rounds other values in their place, can miss the bound.
Values may be sent and summed in bfloat16 or wider, within the bound.
A program may use at most 128 MiB of HBM per device.

```python
import math
import jax
import jax.numpy as jnp
from jax import lax

D = 2048
HEADS = 16
HEAD_DIM = 128
GRID_W = 64
WIN_ROWS = 8
WIN_COLS = 16
ROWS = 384
TOKENS = 24576
CTX = 1024


def draw_query_gain(key, part):
    local = jax.random.fold_in(key, 11)
    values = jax.random.uniform(local, (HEAD_DIM,), jnp.float32, 0.6, 1.4)
    return values


def draw_key_gain(key, part):
    local = jax.random.fold_in(key, 23)
    values = jax.random.uniform(local, (HEAD_DIM,), jnp.float32, 0.6, 1.4)
    return values


def draw_context_bias(key, part):
    local = jax.random.fold_in(key, 37)
    level = math.log(float(WIN_ROWS * WIN_COLS) / float(CTX))
    values = jax.random.uniform(local, (HEADS,), jnp.float32, -2.0, -0.5)
    return values + level


def levels(rng, dims, cuts, smallest, high):
    loudness, own = 1.0, jax.random.fold_in(rng, 6)
    for position, shards_of in cuts:
        draws = jnp.exp(jax.random.uniform(jax.random.fold_in(own, position), (shards_of,), jnp.float32, smallest / len(cuts), high / len(cuts)))
        loudness = loudness * jnp.repeat(draws, dims[position] // shards_of).reshape([-1 if axis == position else 1 for axis in range(len(dims))])
    return loudness


def scatter_about(key, extent, scale, most, cuts=(), kind=jnp.bfloat16):
    drawn = scale * jax.random.normal(key, extent, jnp.float32)
    if cuts:
        drawn = drawn * levels(key, extent, cuts, -0.22, 0.18)
    return jnp.clip(drawn, -most, most).astype(kind)


def setup_inputs(seed: int = 0) -> dict:
    streams_of = jax.random.split(jax.random.key(seed), 16)
    return {
        "resid": scatter_about(streams_of[0], (TOKENS, D), 1.0, 6.0, ((0, 128),)),
        "cond": scatter_about(streams_of[1], (D,), 1.0, 6.0, ((0, 16),)),
        "mod_shift": scatter_about(streams_of[2], (D, D), D ** -0.5, 0.125, ((0, 16), (1, 8))),
        "mod_scale": scatter_about(streams_of[3], (D, D), D ** -0.5, 0.125, ((0, 16), (1, 8))),
        "mod_gate": scatter_about(streams_of[4], (D, D), D ** -0.5, 0.125, ((0, 16), (1, 8))),
        "norm_gain": jnp.clip(1.0 + 0.18 * jax.random.normal(streams_of[5], (D,), jnp.float32), 0.1, 1.9),
        "context": scatter_about(streams_of[6], (CTX, D), 1.0, 6.0, ((0, 16),)),
        "w_query": scatter_about(streams_of[7], (D, HEADS * HEAD_DIM), D ** -0.5, 0.125, ((1, 8),)),
        "w_key": scatter_about(streams_of[8], (D, HEADS * HEAD_DIM), D ** -0.5, 0.125, ((1, 8),)),
        "w_value": scatter_about(streams_of[9], (D, HEADS * HEAD_DIM), D ** -0.5, 0.125, ((1, 8),)),
        "query_gain": draw_query_gain(jax.random.fold_in(streams_of[15], 71), 0),
        "key_gain": draw_key_gain(jax.random.fold_in(streams_of[15], 71), 0),
        "offset_bias": scatter_about(streams_of[12], (HEADS, 2 * WIN_ROWS - 1, 2 * WIN_COLS - 1), 1.0, 4.0, ((0, 8),), jnp.float32),
        "context_bias": draw_context_bias(jax.random.fold_in(streams_of[15], 71), 0),
        "w_out": scatter_about(streams_of[14], (HEADS * HEAD_DIM, D), (HEADS * HEAD_DIM // 16) ** -0.5, 0.5),
    }


EPS = 1e-06

def widen(values):
    return lax.optimization_barrier(values).astype(jnp.float32)

def normed_heads(values, gain):
    count = values.shape[0]
    split = values.reshape(count, HEADS, HEAD_DIM)
    scaled = split * lax.rsqrt(lax.optimization_barrier(jnp.mean(split * split, axis=-1, keepdims=True)) + EPS) * gain.astype(jnp.float32)
    return scaled.reshape(count, HEADS * HEAD_DIM).astype(jnp.bfloat16)

def reference(resid, cond, mod_shift, mod_scale, mod_gate, norm_gain, context, w_query, w_key, w_value, query_gain, key_gain, offset_bias, context_bias, w_out):
    lifted = jax.nn.silu(cond.astype(jnp.float32)).astype(jnp.bfloat16)
    shift = jnp.dot(lifted, mod_shift, preferred_element_type=jnp.float32)
    scale = jnp.dot(lifted, mod_scale, preferred_element_type=jnp.float32)
    gate = jnp.dot(lifted, mod_gate, preferred_element_type=jnp.float32)
    floats = resid.astype(jnp.float32)
    inverse = lax.rsqrt(lax.optimization_barrier(jnp.mean(floats * floats, axis=-1, keepdims=True)) + EPS)
    normed = (floats * inverse * norm_gain.astype(jnp.float32) * (1.0 + scale) + shift).astype(jnp.bfloat16)
    query = normed_heads(jnp.dot(normed, w_query, preferred_element_type=jnp.float32), query_gain)
    key = normed_heads(jnp.dot(normed, w_key, preferred_element_type=jnp.float32), key_gain)
    value = jnp.dot(normed, w_value, preferred_element_type=jnp.float32).astype(jnp.bfloat16)
    ctx_floats = context.astype(jnp.float32)
    ctx_inverse = lax.rsqrt(lax.optimization_barrier(jnp.mean(ctx_floats * ctx_floats, axis=-1, keepdims=True)) + EPS)
    ctx_normed = (ctx_floats * ctx_inverse * norm_gain.astype(jnp.float32)).astype(jnp.bfloat16)
    ctx_key = normed_heads(jnp.dot(ctx_normed, w_key, preferred_element_type=jnp.float32), key_gain)
    ctx_value = jnp.dot(ctx_normed, w_value, preferred_element_type=jnp.float32).astype(jnp.bfloat16)
    ctx_key = widen(ctx_key).reshape(CTX, HEADS, HEAD_DIM)
    ctx_value = widen(ctx_value).reshape(CTX, HEADS, HEAD_DIM)
    q_grid = widen(query).reshape(ROWS, GRID_W, HEADS, HEAD_DIM)
    k_grid = widen(key).reshape(ROWS, GRID_W, HEADS, HEAD_DIM)
    v_grid = widen(value).reshape(ROWS, GRID_W, HEADS, HEAD_DIM)
    columns = jnp.arange(GRID_W, dtype=jnp.int32)
    col_start = jnp.clip(columns - WIN_COLS // 2, 0, GRID_W - WIN_COLS)
    valid = (columns[None, :] >= col_start[:, None]) & (columns[None, :] < col_start[:, None] + WIN_COLS)
    col_offset = jnp.clip(columns[None, :] - columns[:, None] + WIN_COLS - 1, 0, 2 * WIN_COLS - 2)
    bias_table = offset_bias.astype(jnp.float32)
    ctx_shift = context_bias.astype(jnp.float32)[:, None, None]
    factor = HEAD_DIM ** (-0.5)

    def one_row(row):
        start = jnp.clip(row - WIN_ROWS // 2, 0, ROWS - WIN_ROWS).astype(jnp.int32)
        queries = lax.dynamic_index_in_dim(q_grid, row, 0, keepdims=False)
        keys = lax.dynamic_slice_in_dim(k_grid, start, WIN_ROWS, 0)
        values = lax.dynamic_slice_in_dim(v_grid, start, WIN_ROWS, 0)
        row_offset = (start + jnp.arange(WIN_ROWS, dtype=jnp.int32) - row + WIN_ROWS - 1).astype(jnp.int32)
        bias = bias_table[:, row_offset][:, :, col_offset]
        s_win = jnp.einsum('qhd,rkhd->hqrk', queries, keys) * factor + jnp.transpose(bias, (0, 2, 1, 3))
        s_win = jnp.where(valid[None, :, None, :], s_win, -1e+30).reshape(HEADS, GRID_W, WIN_ROWS * GRID_W)
        s_ctx = jnp.einsum('qhd,chd->hqc', queries, ctx_key) * factor + ctx_shift
        probs = jax.nn.softmax(jnp.concatenate([s_win, s_ctx], axis=-1), axis=-1).astype(jnp.bfloat16)
        probs = widen(probs)
        p_win = probs[:, :, :WIN_ROWS * GRID_W].reshape(HEADS, GRID_W, WIN_ROWS, GRID_W)
        p_ctx = probs[:, :, WIN_ROWS * GRID_W:]
        out = jnp.einsum('hqrk,rkhd->qhd', p_win, values) + jnp.einsum('hqc,chd->qhd', p_ctx, ctx_value)
        return out.astype(jnp.bfloat16).reshape(GRID_W, HEADS * HEAD_DIM)
    attended = lax.map(one_row, jnp.arange(ROWS, dtype=jnp.int32)).reshape(TOKENS, HEADS * HEAD_DIM)
    projected = jnp.dot(attended, w_out, preferred_element_type=jnp.float32)
    return (floats + gate * projected).astype(jnp.bfloat16)
```

```python
import functools

import jax
import jax.numpy as jnp
from jax import lax
from jax.experimental import pallas as pl
from jax.experimental.pallas import tpu as pltpu
from jax.sharding import Mesh
from jax.sharding import PartitionSpec as P

MESH = pl.DeviceIdType.MESH
BF16, F32 = jnp.bfloat16, jnp.float32
EPS = 1e-06
LOG2E = 1.4426950408889634
HEAD = 128
GRID_W = 64
D = 2048
CTX = 1024
ROWS_DEV = 24
TOK = 1536
SHARD = 192
HALF = 96
WIDE = 256
NEG = -1e30
NT = (((1,), (1,)), ((), ()))


def dot_nt(a, b):
    return lax.dot_general(a, b, NT, preferred_element_type=F32)


def dot(a, b):
    return jnp.dot(a, b, preferred_element_type=F32)


def inv_rms(v):
    return lax.rsqrt(jnp.mean(v * v, axis=-1, keepdims=True) + EPS)


def kernel(
    resid, cond, mod_shift, mod_scale, mod_gate, norm_gain, context, w_query, w_key, w_value,
    query_gain, key_gain, offset_bias, context_bias, w_out, out,
    G, WQ, WK, WV, WO, CX, NRM, R, Q, KV, CKV, MP, MS, MSUM, MOD, OB, T2, S, PR, L, ATT, RX,
    load_sem, ag_send, ag_recv, mp_send, mp_recv, ms_send, ms_recv, cx_send, cx_recv,
    halo_send, halo_recv, aa_send, aa_recv,
):
    z, y, x, c = (lax.axis_index(a) for a in ("z", "y", "x", "c"))
    sp, tp = z * 4 + y, x * 2 + c
    right, left, opp, mate = (x + 1) % 4, (x + 3) % 4, (x + 2) % 4, 1 - c

    def sp_dev(s):
        return (s // 4, s % 4, x, c)

    def tp_dev(t):
        return (z, y, t // 2, t % 2)

    loads = [
        pltpu.make_async_copy(resid.at[pl.ds(0, HALF)], G.at[tp * 2], load_sem.at[0]),
        pltpu.make_async_copy(resid.at[pl.ds(HALF, HALF)], G.at[tp * 2 + 1], load_sem.at[1]),
        pltpu.make_async_copy(context, CX, load_sem.at[2]),
        pltpu.make_async_copy(w_key, WK, load_sem.at[3]),
        pltpu.make_async_copy(w_value, WV, load_sem.at[4]),
        pltpu.make_async_copy(w_query, WQ, load_sem.at[5]),
        pltpu.make_async_copy(w_out, WO, load_sem.at[6]),
    ]
    for one in loads:
        one.start()

    barrier = pltpu.get_barrier_semaphore()

    @pl.loop(1, 8)
    def _(k):
        pl.semaphore_signal(barrier, inc=1, device_id=tp_dev((tp + k) % 8), device_id_type=MESH)

    @pl.loop(1, 16)
    def _(k):
        pl.semaphore_signal(barrier, inc=1, device_id=sp_dev((sp + k) % 16), device_id_type=MESH)

    pl.semaphore_wait(barrier, 22)

    def ag_copy(chunk, slot, device):
        return pltpu.make_async_remote_copy(
            src_ref=G.at[chunk], dst_ref=G.at[chunk], send_sem=ag_send.at[slot],
            recv_sem=ag_recv.at[chunk], device_id=device, device_id_type=MESH,
        )

    to_right, to_left, to_mate = (z, y, right, c), (z, y, left, c), (z, y, x, mate)
    loads[0].wait()
    loads[1].wait()
    ag_copy(tp * 2, 0, to_right).start()
    ag_copy(tp * 2 + 1, 1, to_left).start()
    ag_copy(tp * 2, 2, to_mate).start()
    ag_copy(tp * 2 + 1, 3, to_mate).start()
    ag_copy(tp * 2 + 1, 4, to_right).start()
    ag_copy(tp * 2, 5, to_left).start()

    cf = cond[...].astype(F32)
    lifted = jnp.broadcast_to(cf / (1.0 + jnp.exp(-cf)), (16, 128)).astype(BF16)
    rows8 = lax.broadcasted_iota(jnp.int32, (8, WIDE), 0)
    p_shift = dot(lifted, mod_shift[...])[0:8]
    p_scale = dot(lifted, mod_scale[...])[0:8]
    p_gate = dot(lifted, mod_gate[...])[0:8]
    MP[sp] = jnp.where(rows8 == 0, p_shift, jnp.where(rows8 == 1, p_scale, p_gate))

    def mp_copy(k):
        return pltpu.make_async_remote_copy(
            src_ref=MP.at[sp], dst_ref=MP.at[sp], send_sem=mp_send.at[k],
            recv_sem=mp_recv.at[sp], device_id=sp_dev((sp + k) % 16), device_id_type=MESH,
        )

    def mp_wait(k):
        s = (sp + k) % 16
        return pltpu.make_async_remote_copy(
            src_ref=MP.at[s], dst_ref=MP.at[s], send_sem=mp_send.at[k],
            recv_sem=mp_recv.at[s], device_id=sp_dev(s), device_id_type=MESH,
        )

    @pl.loop(1, 16)
    def _(k):
        mp_copy(k).start()

    loads[2].wait()

    @pl.loop(0, 4)
    def _(i):
        rows = pl.ds(pl.multiple_of(i * 16, 16), 16)
        v = CX[rows, :].astype(F32)
        NRM[rows, :] = (v * inv_rms(v) * norm_gain[...]).astype(BF16)

    loads[3].wait()
    loads[4].wait()
    kg, qg = key_gain[...], query_gain[...]
    ck = dot(NRM[0:64, :], WK[...])
    cv = dot(NRM[0:64, :], WV[...])
    own_ctx = pl.ds(pl.multiple_of(sp * 64, 64), 64)
    for h in range(2):
        part = ck[:, h * HEAD : (h + 1) * HEAD]
        CKV[own_ctx, h * HEAD : (h + 1) * HEAD] = (part * inv_rms(part) * kg).astype(BF16)
    CKV[own_ctx, WIDE:] = cv.astype(BF16)

    def cx_copy(s, k):
        rows = pl.ds(pl.multiple_of(s * 64, 64), 64)
        return pltpu.make_async_remote_copy(
            src_ref=CKV.at[rows], dst_ref=CKV.at[rows], send_sem=cx_send.at[k],
            recv_sem=cx_recv.at[s], device_id=sp_dev((sp + k) % 16), device_id_type=MESH,
        )

    @pl.loop(1, 16)
    def _(k):
        cx_copy(sp, k).start()

    @pl.loop(1, 16)
    def _(k):
        mp_wait(k).wait_recv()

    total = MP[0]
    for s in range(1, 16):
        total = total + MP[s]
    MS[tp] = total

    def ms_copy(t, k):
        return pltpu.make_async_remote_copy(
            src_ref=MS.at[t], dst_ref=MS.at[t], send_sem=ms_send.at[k],
            recv_sem=ms_recv.at[t], device_id=tp_dev((tp + k) % 8), device_id_type=MESH,
        )

    @pl.loop(1, 8)
    def _(k):
        ms_copy(tp, k).start()

    OB[...] = jnp.zeros_like(OB)
    for h in range(2):
        OB[h, 0:15, 0:31] = offset_bias[h] * LOG2E
    col = lax.broadcasted_iota(jnp.int32, (GRID_W, 128), 0)
    lane = lax.broadcasted_iota(jnp.int32, (GRID_W, 128), 1)
    key_col = lane % GRID_W
    begin = jnp.clip(col - 8, 0, GRID_W - 16)
    valid = (key_col >= begin) & (key_col < begin + 16)
    for h in range(2):

        @pl.loop(0, 14)
        def _(o):
            one = jnp.broadcast_to(OB[h, pl.ds(o, 1), :], (GRID_W, 128))
            two = jnp.broadcast_to(OB[h, pl.ds(o + 1, 1), :], (GRID_W, 128))
            one = pltpu.roll(one, 113, 1, stride=1, stride_axis=0)
            two = pltpu.roll(two, 49, 1, stride=1, stride_axis=0)
            T2[h, o] = jnp.where(valid, jnp.where(lane < GRID_W, one, two), NEG)

    @pl.loop(1, 8)
    def _(k):
        ms_copy((tp + k) % 8, k).wait_recv()

    for t in range(8):
        cols = slice(t * WIDE, (t + 1) * WIDE)
        block = MS[t]
        MOD[0:1, cols] = block[0:1]
        MOD[1:2, cols] = norm_gain[:, cols] * (1.0 + block[1:2])
        MOD[2:3, cols] = block[2:3]

    loads[5].wait()

    @pl.loop(0, 4)
    def _(r):
        flip = jnp.where(r == 2, 1, 0)

        def chunk_of(j):
            side = j % 2
            dx = jnp.where(r == 0, 0, jnp.where(r == 3, 2, 3 - 2 * side))
            core = c if j < 2 else mate
            return (((x + dx) % 4) * 2 + core) * 2 + (side + flip) % 2

        @pl.when(r > 0)
        def _():
            for j in range(2):
                chunk = chunk_of(j)
                ag_copy(chunk, 0, to_right).wait_recv()
                ag_copy(chunk, 6 + 2 * r + j, to_mate).start()
                @pl.when(r == 1)
                def _():
                    ag_copy(chunk, 6 + j, to_right if j == 0 else to_left).start()

        for j in range(4):
            chunk = chunk_of(j)
            if j >= 2:
                ag_copy(chunk, 0, to_right).wait_recv()

            @pl.loop(0, 6)
            def _(i):
                rows = pl.ds(pl.multiple_of(i * 16, 16), 16)
                v = G[chunk, rows, :].astype(F32)
                v = v * inv_rms(v) * MOD[1:2, :] + MOD[0:1, :]
                NRM[pl.ds(pl.multiple_of(j * HALF + i * 16, 16), 16), :] = v.astype(BF16)

        for k, w in enumerate((WQ, WK, WV)):
            R[:, k * WIDE : (k + 1) * WIDE] = dot(NRM[...], w[...])
        for j in range(4):
            chunk = chunk_of(j)

            @pl.loop(0, 6)
            def _(i):
                rows = pl.ds(pl.multiple_of(j * HALF + i * 16, 16), 16)
                q_rows = pl.ds(pl.multiple_of(chunk * HALF + i * 16, 16), 16)
                k_rows = pl.ds(pl.multiple_of(chunk * HALF + i * 16 + 4 * GRID_W, 16), 16)
                for h in range(2):
                    a, b = h * HEAD, (h + 1) * HEAD
                    part = R[rows, a:b]
                    Q[q_rows, a:b] = (part * inv_rms(part) * qg).astype(BF16)
                    part = R[rows, WIDE + a : WIDE + b]
                    KV[k_rows, a:b] = (part * inv_rms(part) * kg).astype(BF16)
                KV[k_rows, WIDE:] = R[rows, 2 * WIDE :].astype(BF16)

    EDGE = 4 * GRID_W

    def halo_copy(src, dst, k, s):
        return pltpu.make_async_remote_copy(
            src_ref=KV.at[pl.ds(src, EDGE)], dst_ref=KV.at[pl.ds(dst, EDGE)],
            send_sem=halo_send.at[k], recv_sem=halo_recv.at[k],
            device_id=sp_dev(s), device_id_type=MESH,
        )

    halos = (
        halo_copy(EDGE, 28 * GRID_W, 0, (sp + 15) % 16),
        halo_copy(24 * GRID_W, 0, 1, (sp + 1) % 16),
    )
    for one in halos:
        one.start()

    @pl.loop(1, 16)
    def _(k):
        cx_copy((sp + k) % 16, k).wait_recv()

    for one in halos:
        one.wait_recv()

    lo = jnp.where(sp == 0, 4, 0)
    hi = jnp.where(sp == 15, 20, 24)
    factor = HEAD**-0.5 * LOG2E

    def aa_copy(t, src, k):
        return pltpu.make_async_remote_copy(
            src_ref=ATT.at[t], dst_ref=RX.at[src], send_sem=aa_send.at[k],
            recv_sem=aa_recv.at[src], device_id=tp_dev(t), device_id_type=MESH,
        )

    @pl.loop(1, 9)
    def _(k):
        t = (tp + k) % 8
        base = pl.multiple_of(t * SHARD, SHARD)
        for h in range(2):
            a, b = h * HEAD, (h + 1) * HEAD
            cb = context_bias[h] * LOG2E
            S[:, 0:CTX] = dot_nt(Q[pl.ds(base, SHARD), a:b], CKV[:, a:b])
            keys = []
            for i in range(3):
                row = t * 3 + i
                start = jnp.minimum(jnp.maximum(row, lo), hi)
                keys.append((pl.ds(pl.multiple_of(start * GRID_W, GRID_W), 512), start - row + 3))
                S[i * 64 : (i + 1) * 64, CTX:] = dot_nt(
                    Q[pl.ds(base + i * 64, 64), a:b], KV[keys[i][0], a:b]
                )
            for i in range(3):
                offset = keys[i][1]

                @pl.loop(0, 4)
                def _(j):
                    rows = pl.ds(pl.multiple_of(i * 64 + j * 16, 16), 16)
                    sub = pl.ds(pl.multiple_of(j * 16, 16), 16)
                    zc = S[rows, 0:CTX] * factor
                    bias = jnp.concatenate([T2[h, offset + 2 * n, sub, :] for n in range(4)], axis=1)
                    zw = S[rows, CTX:] * factor + bias
                    top = jnp.maximum(
                        jnp.max(zc, axis=1, keepdims=True) + cb, jnp.max(zw, axis=1, keepdims=True)
                    )
                    pc = jnp.exp2(zc - (top - cb))
                    pw = jnp.exp2(zw - top)
                    norm = jnp.sum(pc, axis=1, keepdims=True) + jnp.sum(pw, axis=1, keepdims=True)
                    PR[rows, 0:CTX] = pc.astype(BF16)
                    PR[rows, CTX:] = pw.astype(BF16)
                    L[rows, :] = jnp.broadcast_to(1.0 / norm, (16, HEAD))

            acc = dot(PR[:, 0:CTX], CKV[:, WIDE + a : WIDE + b])
            for i in range(3):
                part = slice(i * 64, (i + 1) * 64)
                full = acc[part] + dot(PR[part, CTX:], KV[keys[i][0], WIDE + a : WIDE + b])
                ATT[t, part, a:b] = (full * L[part, :]).astype(BF16)

        @pl.when(k < 8)
        def _():
            aa_copy(t, tp, k).start()

    @pl.loop(1, 8)
    def _(k):
        aa_copy(tp, (tp + k) % 8, k).wait_recv()

    RX[tp] = ATT[tp]
    loads[6].wait()

    @pl.loop(0, 8)
    def _(n):
        cols = pl.ds(pl.multiple_of(n * WIDE, WIDE), WIDE)
        acc = dot(RX[0], WO[0:WIDE, cols])
        for t in range(1, 8):
            acc = acc + dot(RX[t], WO[t * WIDE : (t + 1) * WIDE, cols])
        for s in range(2):
            part = slice(s * HALF, (s + 1) * HALF)
            own = G[tp * 2 + s, :, cols].astype(F32)
            out[part, cols] = (own + MOD[2:3, cols] * acc[part]).astype(BF16)

    for slot in range(14):
        ag_copy(tp * 2, slot, to_mate).wait_send()

    @pl.loop(1, 16)
    def _(k):
        mp_copy(k).wait_send()
        cx_copy(sp, k).wait_send()

    @pl.loop(1, 8)
    def _(k):
        ms_copy(tp, k).wait_send()
        aa_copy((tp + k) % 8, tp, k).wait_send()

    for one in halos:
        one.wait_send()


def shards(
    resid, cond, mod_shift, mod_scale, mod_gate, norm_gain, context, w_query, w_key, w_value,
    query_gain, key_gain, offset_bias, context_bias, w_out,
):
    vmem = pl.BlockSpec(memory_space=pltpu.VMEM)
    smem = pl.BlockSpec(memory_space=pltpu.SMEM)
    hbm = pl.BlockSpec(memory_space=pl.ANY)
    dma = pltpu.SemaphoreType.DMA
    scratch = [
        pltpu.VMEM((16, HALF, D), BF16),
        pltpu.VMEM((D, WIDE), BF16),
        pltpu.VMEM((D, WIDE), BF16),
        pltpu.VMEM((D, WIDE), BF16),
        pltpu.VMEM((D, D), BF16),
        pltpu.VMEM((64, D), BF16),
        pltpu.VMEM((4 * HALF, D), BF16),
        pltpu.VMEM((4 * HALF, 3 * WIDE), F32),
        pltpu.VMEM((TOK, WIDE), BF16),
        pltpu.VMEM((TOK + 512, 2 * WIDE), BF16),
        pltpu.VMEM((CTX, 2 * WIDE), BF16),
        pltpu.VMEM((16, 8, WIDE), F32),
        pltpu.VMEM((8, 8, WIDE), F32),
        pltpu.VMEM((8, WIDE), F32),
        pltpu.VMEM((8, D), F32),
        pltpu.VMEM((2, 16, 128), F32),
        pltpu.VMEM((2, 14, GRID_W, 128), F32),
        pltpu.VMEM((SHARD, CTX + 512), F32),
        pltpu.VMEM((SHARD, CTX + 512), BF16),
        pltpu.VMEM((SHARD, HEAD), F32),
        pltpu.VMEM((8, SHARD, WIDE), BF16),
        pltpu.VMEM((8, SHARD, WIDE), BF16),
        dma((7,)), dma((14,)), dma((16,)), dma((16,)), dma((16,)), dma((8,)), dma((8,)),
        dma((16,)), dma((16,)), dma((2,)), dma((2,)), dma((8,)), dma((8,)),
    ]
    return pl.pallas_call(
        kernel,
        out_shape=jax.ShapeDtypeStruct((SHARD, D), BF16),
        in_specs=[hbm, vmem, vmem, vmem, vmem, vmem, hbm, hbm, hbm, hbm, vmem, vmem, vmem, smem, hbm],
        out_specs=vmem,
        scratch_shapes=scratch,
        compiler_params=pltpu.CompilerParams(
            collective_id=0, has_side_effects=True, vmem_limit_bytes=60 * 1024 * 1024
        ),
    )(
        resid, cond.reshape(1, -1), mod_shift, mod_scale, mod_gate, norm_gain.reshape(1, -1),
        context, w_query, w_key, w_value, query_gain.reshape(1, -1), key_gain.reshape(1, -1),
        offset_bias, context_bias, w_out,
    )


def solution(mesh):
    grid = Mesh(mesh.devices.reshape(4, 4, 4, 2), ("z", "y", "x", "c"))
    sp, tp, both = ("z", "y"), ("x", "c"), ("z", "y", "x", "c")
    placed = (
        P(both, None), P(sp), P(sp, tp), P(sp, tp), P(sp, tp), P(), P(sp, None),
        P(None, tp), P(None, tp), P(None, tp), P(), P(), P(tp, None, None), P(tp), P(),
    )
    return jax.shard_map(
        shards, mesh=grid, in_specs=placed, out_specs=P(both, None), check_vma=False
    )
```

```python
import functools

import jax
import jax.numpy as jnp
from jax import lax
from jax.experimental import pallas as pl
from jax.experimental.pallas import tpu as pltpu
from jax.sharding import Mesh
from jax.sharding import PartitionSpec as P

MESH = pl.DeviceIdType.MESH
BF16, F32 = jnp.bfloat16, jnp.float32
EPS = 1e-06
LOG2E = 1.4426950408889634
HEAD = 128
GRID_W = 64
D = 2048
CTX = 1024
ROWS_DEV = 24
TOK = 1536
SHARD = 192
HALF = 96
QUART = 48
WIDE = 256
NEG = -1e30
NT = (((1,), (1,)), ((), ()))


def dot_nt(a, b):
    return lax.dot_general(a, b, NT, preferred_element_type=F32)


def dot(a, b):
    return jnp.dot(a, b, preferred_element_type=F32)


def inv_rms(v):
    return lax.rsqrt(jnp.mean(v * v, axis=-1, keepdims=True) + EPS)


def kernel(
    resid, cond, mod_shift, mod_scale, mod_gate, norm_gain, context, w_query, w_key, w_value,
    query_gain, key_gain, offset_bias, context_bias, w_out, out,
    G, WQ, WK, WV, WO, CX, NRM, R, Q, KV, CKV, MP, MS, MSUM, MOD, OB, T2, S, PR, M, L2, L, ATT, RX,
    load_sem, ag_send, ag_recv, mp_send, mp_recv, ms_send, ms_recv, cx_send, cx_recv,
    halo_send, halo_recv, aa_send, aa_recv,
):
    z, y, x, c = (lax.axis_index(a) for a in ("z", "y", "x", "c"))
    sp, tp = z * 4 + y, x * 2 + c
    right, left, opp, mate = (x + 1) % 4, (x + 3) % 4, (x + 2) % 4, 1 - c

    def sp_dev(s):
        return (s // 4, s % 4, x, c)

    def tp_dev(t):
        return (z, y, t // 2, t % 2)

    with jax.named_scope("entry"):
        loads = [
            pltpu.make_async_copy(
                resid.at[pl.ds(n * QUART, QUART)], G.at[tp * 4 + n], load_sem.at[n]
            )
            for n in range(4)
        ] + [
            pltpu.make_async_copy(context, CX, load_sem.at[4]),
            pltpu.make_async_copy(w_key, WK, load_sem.at[5]),
            pltpu.make_async_copy(w_value, WV, load_sem.at[6]),
            pltpu.make_async_copy(w_query, WQ, load_sem.at[7]),
            pltpu.make_async_copy(w_out, WO, load_sem.at[8]),
        ]
        for one in loads:
            one.start()

        barrier = pltpu.get_barrier_semaphore()

        @pl.loop(1, 8)
        def _(k):
            pl.semaphore_signal(barrier, inc=1, device_id=tp_dev((tp + k) % 8), device_id_type=MESH)

        @pl.loop(1, 16)
        def _(k):
            pl.semaphore_signal(barrier, inc=1, device_id=sp_dev((sp + k) % 16), device_id_type=MESH)

        pl.semaphore_wait(barrier, 22)

    def ag_copy(chunk, slot, device):
        return pltpu.make_async_remote_copy(
            src_ref=G.at[chunk], dst_ref=G.at[chunk], send_sem=ag_send.at[slot],
            recv_sem=ag_recv.at[chunk], device_id=device, device_id_type=MESH,
        )

    to_right, to_left, to_mate = (z, y, right, c), (z, y, left, c), (z, y, x, mate)
    to_right, to_left, to_mate = (z, y, right, c), (z, y, left, c), (z, y, x, mate)
    own = tp * 4
    for n in range(4):
        loads[n].wait()
    ag_copy(own, 0, to_right).start()
    ag_copy(own + 3, 4, to_left).start()
    for n in range(4):
        ag_copy(own + n, 8 + n, to_mate).start()

    cf = cond[...].astype(F32)
    lifted = jnp.broadcast_to(cf / (1.0 + jnp.exp(-cf)), (16, 128)).astype(BF16)
    rows8 = lax.broadcasted_iota(jnp.int32, (8, WIDE), 0)
    p_shift = dot(lifted, mod_shift[...])[0:8]
    p_scale = dot(lifted, mod_scale[...])[0:8]
    p_gate = dot(lifted, mod_gate[...])[0:8]
    MP[sp] = jnp.where(rows8 == 0, p_shift, jnp.where(rows8 == 1, p_scale, p_gate))

    def mp_copy(k):
        return pltpu.make_async_remote_copy(
            src_ref=MP.at[sp], dst_ref=MP.at[sp], send_sem=mp_send.at[k],
            recv_sem=mp_recv.at[sp], device_id=sp_dev((sp + k) % 16), device_id_type=MESH,
        )

    def mp_wait(k):
        s = (sp + k) % 16
        return pltpu.make_async_remote_copy(
            src_ref=MP.at[s], dst_ref=MP.at[s], send_sem=mp_send.at[k],
            recv_sem=mp_recv.at[s], device_id=sp_dev(s), device_id_type=MESH,
        )

    @pl.loop(1, 16)
    def _(k):
        mp_copy(k).start()

    loads[4].wait()

    @pl.loop(0, 4)
    def _(i):
        rows = pl.ds(pl.multiple_of(i * 16, 16), 16)
        v = CX[rows, :].astype(F32)
        NRM[rows, :] = (v * inv_rms(v) * norm_gain[...]).astype(BF16)

    loads[5].wait()
    loads[6].wait()
    kg, qg = key_gain[...], query_gain[...]
    ck = dot(NRM[0:64, :], WK[...])
    cv = dot(NRM[0:64, :], WV[...])
    own_ctx = pl.ds(pl.multiple_of(sp * 64, 64), 64)
    for h in range(2):
        part = ck[:, h * HEAD : (h + 1) * HEAD]
        CKV[own_ctx, h * HEAD : (h + 1) * HEAD] = (part * inv_rms(part) * kg).astype(BF16)
    CKV[own_ctx, WIDE:] = cv.astype(BF16)

    def cx_copy(s, k):
        rows = pl.ds(pl.multiple_of(s * 64, 64), 64)
        return pltpu.make_async_remote_copy(
            src_ref=CKV.at[rows], dst_ref=CKV.at[rows], send_sem=cx_send.at[k],
            recv_sem=cx_recv.at[s], device_id=sp_dev((sp + k) % 16), device_id_type=MESH,
        )

    @pl.loop(1, 16)
    def _(k):
        cx_copy(sp, k).start()

    with jax.named_scope("mp_wait"):
        @pl.loop(1, 16)
        def _(k):
            mp_wait(k).wait_recv()

    total = MP[0]
    for s in range(1, 16):
        total = total + MP[s]
    MS[tp] = total

    def ms_copy(t, k):
        return pltpu.make_async_remote_copy(
            src_ref=MS.at[t], dst_ref=MS.at[t], send_sem=ms_send.at[k],
            recv_sem=ms_recv.at[t], device_id=tp_dev((tp + k) % 8), device_id_type=MESH,
        )

    @pl.loop(1, 8)
    def _(k):
        ms_copy(tp, k).start()

    for n in range(1, 4):
        ag_copy(own + n, n, to_right).start()
        ag_copy(own + 3 - n, 4 + n, to_left).start()

    with jax.named_scope("bias"):
        OB[...] = jnp.zeros_like(OB)
        for h in range(2):
            OB[h, 0:15, 0:31] = offset_bias[:, h, :] * LOG2E
        col = lax.broadcasted_iota(jnp.int32, (GRID_W, 128), 0)
        lane = lax.broadcasted_iota(jnp.int32, (GRID_W, 128), 1)
        key_col = lane % GRID_W
        begin = jnp.clip(col - 8, 0, GRID_W - 16)
        valid = (key_col >= begin) & (key_col < begin + 16)
        for h in range(2):

            @pl.loop(0, 14)
            def _(o):
                one = jnp.broadcast_to(OB[h, pl.ds(o, 1), :], (GRID_W, 128))
                two = jnp.broadcast_to(OB[h, pl.ds(o + 1, 1), :], (GRID_W, 128))
                one = pltpu.roll(one, 113, 1, stride=1, stride_axis=0)
                two = pltpu.roll(two, 49, 1, stride=1, stride_axis=0)
                T2[h, o] = jnp.where(valid, jnp.where(lane < GRID_W, one, two), NEG)

    with jax.named_scope("ms_wait"):
        @pl.loop(1, 8)
        def _(k):
            ms_copy((tp + k) % 8, k).wait_recv()

    for t in range(8):
        cols = slice(t * WIDE, (t + 1) * WIDE)
        block = MS[t]
        MOD[0:1, cols] = block[0:1]
        MOD[1:2, cols] = norm_gain[:, cols] * (1.0 + block[1:2])
        MOD[2:3, cols] = block[2:3]

    loads[7].wait()

    def norm_rows(chunk, at):
        for i in range(HALF // 16):
            v = G[chunk * 2 + i // 3, i % 3 * 16 : i % 3 * 16 + 16, :].astype(F32)
            L[i * 16 : i * 16 + 16, :] = jnp.broadcast_to(inv_rms(v), (16, HEAD))
        for i in range(HALF // 16):
            v = G[chunk * 2 + i // 3, i % 3 * 16 : i % 3 * 16 + 16, :].astype(F32)
            v = v * L[i * 16 : i * 16 + 16, 0:1] * MOD[1:2, :] + MOD[0:1, :]
            NRM[at + i * 16 : at + i * 16 + 16, :] = v.astype(BF16)

    def head_rows(chunk, at):
        for i in range(HALF // 16):
            rows = slice(at + i * 16, at + i * 16 + 16)
            q_rows = pl.ds(pl.multiple_of(chunk * HALF + i * 16, 16), 16)
            k_rows = pl.ds(pl.multiple_of(chunk * HALF + i * 16 + 4 * GRID_W, 16), 16)
            for h in range(2):
                a, b = h * HEAD, (h + 1) * HEAD
                part = R[rows, a:b]
                Q[q_rows, a:b] = (part * inv_rms(part) * qg).astype(BF16)
                part = R[rows, WIDE + a : WIDE + b]
                KV[k_rows, a:b] = (part * inv_rms(part) * kg).astype(BF16)
            KV[k_rows, WIDE:] = R[rows, 2 * WIDE :].astype(BF16)

    @pl.loop(0, 4)
    def _(r):
        flip = jnp.where(r == 2, 1, 0)

        def chunk_of(j):
            side = j % 2
            dx = jnp.where(r == 0, 0, jnp.where(r == 3, 2, 3 - 2 * side))
            core = c if j < 2 else mate
            return (((x + dx) % 4) * 2 + core) * 2 + (side + flip) % 2

        @pl.when(r > 0)
        def _():
            for n in range(2):
                for j in range(2):
                    piece = chunk_of(j) * 2 + (n + j) % 2
                    with jax.named_scope("ring_wait"):
                        ag_copy(piece, 0, to_right).wait_recv()
                    ag_copy(piece, 8 + 4 * r + 2 * j + n, to_mate).start()

                    @pl.when(r == 1)
                    def _():
                        ag_copy(piece, 24 + 2 * j + n, to_right if j == 0 else to_left).start()

        for j in range(4):
            chunk = chunk_of(j)
            if j >= 2:
                with jax.named_scope("mate_wait"):
                    for n in range(2):
                        ag_copy(chunk * 2 + n, 0, to_right).wait_recv()

            norm_rows(chunk, j * HALF)

        with jax.named_scope("qkv"):
            for k, w in enumerate((WQ, WK, WV)):
                R[:, k * WIDE : (k + 1) * WIDE] = dot(NRM[...], w[...])
        for j in range(4):
            head_rows(chunk_of(j), j * HALF)

    EDGE = 4 * GRID_W

    def halo_copy(src, dst, k, s):
        return pltpu.make_async_remote_copy(
            src_ref=KV.at[pl.ds(src, EDGE)], dst_ref=KV.at[pl.ds(dst, EDGE)],
            send_sem=halo_send.at[k], recv_sem=halo_recv.at[k],
            device_id=sp_dev(s), device_id_type=MESH,
        )

    halos = (
        halo_copy(EDGE, 28 * GRID_W, 0, (sp + 15) % 16),
        halo_copy(24 * GRID_W, 0, 1, (sp + 1) % 16),
    )
    for one in halos:
        one.start()

    with jax.named_scope("halo_wait"):
        @pl.loop(1, 16)
        def _(k):
            cx_copy((sp + k) % 16, k).wait_recv()

        for one in halos:
            one.wait_recv()

    lo = jnp.where(sp == 0, 4, 0)
    hi = jnp.where(sp == 15, 20, 24)
    factor = HEAD**-0.5 * LOG2E

    def aa_copy(t, src, k):
        return pltpu.make_async_remote_copy(
            src_ref=ATT.at[t], dst_ref=RX.at[src], send_sem=aa_send.at[k],
            recv_sem=aa_recv.at[src], device_id=tp_dev(t), device_id_type=MESH,
        )

    def lanes(v, op):
        parts = [v[:, n * 128 : (n + 1) * 128] for n in range(v.shape[1] // 128)]
        while len(parts) > 1:
            parts = [op(p, q) for p, q in zip(parts[::2], parts[1::2])] + parts[len(parts) & ~1 :]
        return parts[0]

    def attend(t):
        base = pl.multiple_of(t * SHARD, SHARD)
        keys, offsets = [], []
        for i in range(3):
            row = t * 3 + i
            start = jnp.minimum(jnp.maximum(row, lo), hi)
            keys.append(pl.ds(pl.multiple_of(start * GRID_W, GRID_W), 512))
            offsets.append(start - row + 3)
        for h in range(2):
            a, b = h * HEAD, (h + 1) * HEAD
            S[h, :, 0:CTX] = dot_nt(Q[pl.ds(base, SHARD), a:b], CKV[:, a:b])
            for i in range(3):
                S[h, i * 64 : (i + 1) * 64, CTX:] = dot_nt(
                    Q[pl.ds(base + i * 64, 64), a:b], KV[keys[i], a:b]
                )
        for h in range(2):
            a, b = h * HEAD, (h + 1) * HEAD
            cb = context_bias[h] * LOG2E
            strips = [(i, i * 64 + j * 16, slice(j * 16, j * 16 + 16)) for i in range(3) for j in range(4)]

            def window(i, at, sub):
                bias = [T2[h, offsets[i] + 2 * n, sub, :] for n in range(4)]
                return S[h, at : at + 16, CTX:] * factor + jnp.concatenate(bias, axis=1)

            for i, at, sub in strips:
                top = lanes(S[h, at : at + 16, 0:CTX], jnp.maximum) * factor + cb
                top = jnp.maximum(top, lanes(window(i, at, sub), jnp.maximum))
                M[h, at : at + 16, :] = jnp.broadcast_to(jnp.max(top, axis=1, keepdims=True), (16, 128))
            for i, at, sub in strips:
                top = M[h, at : at + 16, 0:1]
                pc = jnp.exp2(S[h, at : at + 16, 0:CTX] * factor - (top - cb))
                pw = jnp.exp2(window(i, at, sub) - top)
                PR[h, at : at + 16, 0:CTX] = pc.astype(BF16)
                PR[h, at : at + 16, CTX:] = pw.astype(BF16)
                norm = lanes(pc, jnp.add) + lanes(pw, jnp.add)
                norm = jnp.sum(norm, axis=1, keepdims=True)
                L2[h, at : at + 16, :] = jnp.broadcast_to(1.0 / norm, (16, 128))
            acc = dot(PR[h, :, 0:CTX], CKV[:, WIDE + a : WIDE + b])
            for i in range(3):
                part = slice(i * 64, (i + 1) * 64)
                full = acc[part] + dot(PR[h, part, CTX:], KV[keys[i], WIDE + a : WIDE + b])
                ATT[t, part, a:b] = (full * L2[h, part, :]).astype(BF16)

    with jax.named_scope("attention"):
        @pl.loop(1, 9)
        def _(k):
            t = (tp + k) % 8
            attend(t)

            @pl.when(k < 8)
            def _():
                aa_copy(t, tp, k).start()

    with jax.named_scope("aa_wait"):
        @pl.loop(1, 8)
        def _(k):
            aa_copy(tp, (tp + k) % 8, k).wait_recv()

    RX[tp] = ATT[tp]
    loads[8].wait()

    with jax.named_scope("project"):
        @pl.loop(0, 8)
        def _(n):
            cols = pl.ds(pl.multiple_of(n * WIDE, WIDE), WIDE)
            acc = dot(RX[0], WO[0:WIDE, cols])
            for t in range(1, 8):
                acc = acc + dot(RX[t], WO[t * WIDE : (t + 1) * WIDE, cols])
            for s in range(4):
                part = slice(s * QUART, (s + 1) * QUART)
                mine = G[own + s, :, cols].astype(F32)
                out[part, cols] = (mine + MOD[2:3, cols] * acc[part]).astype(BF16)

    with jax.named_scope("drain"):
        for slot in range(28):
            ag_copy(own, slot, to_mate).wait_send()

        @pl.loop(1, 16)
        def _(k):
            mp_copy(k).wait_send()
            cx_copy(sp, k).wait_send()

        @pl.loop(1, 8)
        def _(k):
            ms_copy(tp, k).wait_send()
            aa_copy((tp + k) % 8, tp, k).wait_send()

        for one in halos:
            one.wait_send()


def shards(
    resid, cond, mod_shift, mod_scale, mod_gate, norm_gain, context, w_query, w_key, w_value,
    query_gain, key_gain, offset_bias, context_bias, w_out,
):
    vmem = pl.BlockSpec(memory_space=pltpu.VMEM)
    smem = pl.BlockSpec(memory_space=pltpu.SMEM)
    hbm = pl.BlockSpec(memory_space=pl.ANY)
    dma = pltpu.SemaphoreType.DMA
    scratch = [
        pltpu.VMEM((32, QUART, D), BF16),
        pltpu.VMEM((D, WIDE), BF16),
        pltpu.VMEM((D, WIDE), BF16),
        pltpu.VMEM((D, WIDE), BF16),
        pltpu.VMEM((D, D), BF16),
        pltpu.VMEM((64, D), BF16),
        pltpu.VMEM((4 * HALF, D), BF16),
        pltpu.VMEM((4 * HALF, 3 * WIDE), F32),
        pltpu.VMEM((TOK, WIDE), BF16),
        pltpu.VMEM((TOK + 512, 2 * WIDE), BF16),
        pltpu.VMEM((CTX, 2 * WIDE), BF16),
        pltpu.VMEM((16, 8, WIDE), F32),
        pltpu.VMEM((8, 8, WIDE), F32),
        pltpu.VMEM((8, WIDE), F32),
        pltpu.VMEM((8, D), F32),
        pltpu.VMEM((2, 16, 128), F32),
        pltpu.VMEM((2, 14, GRID_W, 128), F32),
        pltpu.VMEM((2, SHARD, CTX + 512), F32),
        pltpu.VMEM((2, SHARD, CTX + 512), BF16),
        pltpu.VMEM((2, SHARD, HEAD), F32),
        pltpu.VMEM((2, SHARD, HEAD), F32),
        pltpu.VMEM((SHARD, HEAD), F32),
        pltpu.VMEM((8, SHARD, WIDE), BF16),
        pltpu.VMEM((8, SHARD, WIDE), BF16),
        dma((9,)), dma((28,)), dma((32,)), dma((16,)), dma((16,)), dma((8,)), dma((8,)),
        dma((16,)), dma((16,)), dma((2,)), dma((2,)), dma((8,)), dma((8,)),
    ]
    return pl.pallas_call(
        kernel,
        out_shape=jax.ShapeDtypeStruct((SHARD, D), BF16),
        in_specs=[hbm, vmem, vmem, vmem, vmem, vmem, hbm, hbm, hbm, hbm, vmem, vmem, vmem, smem, hbm],
        out_specs=vmem,
        scratch_shapes=scratch,
        compiler_params=pltpu.CompilerParams(
            collective_id=0, has_side_effects=True, vmem_limit_bytes=60 * 1024 * 1024
        ),
    )(
        resid, cond.reshape(1, -1), mod_shift, mod_scale, mod_gate, norm_gain.reshape(1, -1),
        context, w_query, w_key, w_value, query_gain.reshape(1, -1), key_gain.reshape(1, -1),
        jnp.transpose(offset_bias, (1, 0, 2)), context_bias, w_out,
    )


def solution(mesh):
    grid = Mesh(mesh.devices.reshape(4, 4, 4, 2), ("z", "y", "x", "c"))
    sp, tp, both = ("z", "y"), ("x", "c"), ("z", "y", "x", "c")
    placed = (
        P(both, None), P(sp), P(sp, tp), P(sp, tp), P(sp, tp), P(), P(sp, None),
        P(None, tp), P(None, tp), P(None, tp), P(), P(), P(tp, None, None), P(tp), P(),
    )
    return jax.shard_map(
        shards, mesh=grid, in_specs=placed, out_specs=P(both, None), check_vma=False
    )
```

```python
import functools

import jax
import jax.numpy as jnp
from jax import lax
from jax.experimental import pallas as pl
from jax.experimental.pallas import tpu as pltpu
from jax.sharding import Mesh
from jax.sharding import PartitionSpec as P

MESH = pl.DeviceIdType.MESH
BF16, F32 = jnp.bfloat16, jnp.float32
EPS = 1e-06
LOG2E = 1.4426950408889634
HEAD = 128
GRID_W = 64
D = 2048
CTX = 1024
ROWS_DEV = 24
TOK = 1536
SHARD = 192
PAD = 288
HALF = 96
QUART = 48
WIDE = 256
NEG = -1e30
NT = (((1,), (1,)), ((), ()))


def dot_nt(a, b):
    return lax.dot_general(a, b, NT, preferred_element_type=F32)


def dot(a, b):
    return jnp.dot(a, b, preferred_element_type=F32)


def inv_rms(v):
    return lax.rsqrt(jnp.mean(v * v, axis=-1, keepdims=True) + EPS)


def kernel(
    resid, cond, mod_shift, mod_scale, mod_gate, norm_gain, context, w_query, w_key, w_value,
    query_gain, key_gain, offset_bias, context_bias, w_out, out,
    G, WQ, WK, WV, WO, CX, NRM, R, Q, KV, CKV, MP, MS, MSUM, MOD, OB, T2, S, PR, SW, PW, VA, CVA, QN, ACC, MC, LC, M, L, PA, ATT, RX,
    load_sem, ag_send, ag_recv, mp_send, mp_recv, ms_send, ms_recv, cx_send, cx_recv,
    halo_send, halo_recv, aa_send, aa_recv,
):
    z, y, x, c = (lax.axis_index(a) for a in ("z", "y", "x", "c"))
    sp, tp = z * 4 + y, x * 2 + c
    right, left, opp, mate = (x + 1) % 4, (x + 3) % 4, (x + 2) % 4, 1 - c

    def sp_dev(s):
        return (s // 4, s % 4, x, c)

    def tp_dev(t):
        return (z, y, t // 2, t % 2)

    with jax.named_scope("entry"):
        loads = [
            pltpu.make_async_copy(
                resid.at[pl.ds(n * QUART, QUART)], G.at[tp * 4 + n], load_sem.at[n]
            )
            for n in range(4)
        ] + [
            pltpu.make_async_copy(context, CX, load_sem.at[4]),
            pltpu.make_async_copy(w_key, WK, load_sem.at[5]),
            pltpu.make_async_copy(w_value, WV, load_sem.at[6]),
            pltpu.make_async_copy(w_query, WQ, load_sem.at[7]),
            pltpu.make_async_copy(w_out, WO, load_sem.at[8]),
        ]
        for one in loads:
            one.start()

        barrier = pltpu.get_barrier_semaphore()

        @pl.loop(1, 8)
        def _(k):
            pl.semaphore_signal(barrier, inc=1, device_id=tp_dev((tp + k) % 8), device_id_type=MESH)

        @pl.loop(1, 16)
        def _(k):
            pl.semaphore_signal(barrier, inc=1, device_id=sp_dev((sp + k) % 16), device_id_type=MESH)

        pl.semaphore_wait(barrier, 22)

    def ag_copy(chunk, slot, device):
        return pltpu.make_async_remote_copy(
            src_ref=G.at[chunk], dst_ref=G.at[chunk], send_sem=ag_send.at[slot],
            recv_sem=ag_recv.at[chunk], device_id=device, device_id_type=MESH,
        )

    to_right, to_left, to_mate = (z, y, right, c), (z, y, left, c), (z, y, x, mate)
    to_right, to_left, to_mate = (z, y, right, c), (z, y, left, c), (z, y, x, mate)
    own = tp * 4
    for n in range(4):
        loads[n].wait()
    ag_copy(own, 0, to_right).start()
    ag_copy(own + 3, 4, to_left).start()
    for n in range(4):
        ag_copy(own + n, 8 + n, to_mate).start()

    cf = cond[...].astype(F32)
    lifted = jnp.broadcast_to(cf / (1.0 + jnp.exp(-cf)), (16, 128)).astype(BF16)
    rows8 = lax.broadcasted_iota(jnp.int32, (8, WIDE), 0)
    p_shift = dot(lifted, mod_shift[...])[0:8]
    p_scale = dot(lifted, mod_scale[...])[0:8]
    p_gate = dot(lifted, mod_gate[...])[0:8]
    MP[sp] = jnp.where(rows8 == 0, p_shift, jnp.where(rows8 == 1, p_scale, p_gate))

    def mp_copy(k):
        return pltpu.make_async_remote_copy(
            src_ref=MP.at[sp], dst_ref=MP.at[sp], send_sem=mp_send.at[k],
            recv_sem=mp_recv.at[sp], device_id=sp_dev((sp + k) % 16), device_id_type=MESH,
        )

    def mp_wait(k):
        s = (sp + k) % 16
        return pltpu.make_async_remote_copy(
            src_ref=MP.at[s], dst_ref=MP.at[s], send_sem=mp_send.at[k],
            recv_sem=mp_recv.at[s], device_id=sp_dev(s), device_id_type=MESH,
        )

    @pl.loop(1, 16)
    def _(k):
        mp_copy(k).start()

    loads[4].wait()

    @pl.loop(0, 4)
    def _(i):
        rows = pl.ds(pl.multiple_of(i * 16, 16), 16)
        v = CX[rows, :].astype(F32)
        NRM[rows, :] = (v * inv_rms(v) * norm_gain[...]).astype(BF16)

    loads[5].wait()
    loads[6].wait()
    kg, qg = key_gain[...], query_gain[...]
    ck = dot(NRM[0:64, :], WK[...])
    cv = dot(NRM[0:64, :], WV[...])
    own_ctx = pl.ds(pl.multiple_of(sp * 64, 64), 64)
    for h in range(2):
        part = ck[:, h * HEAD : (h + 1) * HEAD]
        CKV[own_ctx, h * HEAD : (h + 1) * HEAD] = (part * inv_rms(part) * kg).astype(BF16)
    CKV[own_ctx, WIDE:] = cv.astype(BF16)

    def cx_copy(s, k):
        rows = pl.ds(pl.multiple_of(s * 64, 64), 64)
        return pltpu.make_async_remote_copy(
            src_ref=CKV.at[rows], dst_ref=CKV.at[rows], send_sem=cx_send.at[k],
            recv_sem=cx_recv.at[s], device_id=sp_dev((sp + k) % 16), device_id_type=MESH,
        )

    @pl.loop(1, 16)
    def _(k):
        cx_copy(sp, k).start()

    with jax.named_scope("mp_wait"):
        @pl.loop(1, 16)
        def _(k):
            mp_wait(k).wait_recv()

    total = MP[0]
    for s in range(1, 16):
        total = total + MP[s]
    MS[tp] = total

    def ms_copy(t, k):
        return pltpu.make_async_remote_copy(
            src_ref=MS.at[t], dst_ref=MS.at[t], send_sem=ms_send.at[k],
            recv_sem=ms_recv.at[t], device_id=tp_dev((tp + k) % 8), device_id_type=MESH,
        )

    @pl.loop(1, 8)
    def _(k):
        ms_copy(tp, k).start()

    for n in range(1, 4):
        ag_copy(own + n, n, to_right).start()
        ag_copy(own + 3 - n, 4 + n, to_left).start()

    with jax.named_scope("bias"):
        OB[...] = jnp.zeros_like(OB)
        for h in range(2):
            OB[h, 0:15, 0:31] = offset_bias[:, h, :] * LOG2E
        col = lax.broadcasted_iota(jnp.int32, (GRID_W, 128), 0)
        lane = lax.broadcasted_iota(jnp.int32, (GRID_W, 128), 1)
        key_col = lane % GRID_W
        begin = jnp.clip(col - 8, 0, GRID_W - 16)
        valid = (key_col >= begin) & (key_col < begin + 16)
        for h in range(2):

            @pl.loop(0, 14)
            def _(o):
                one = jnp.broadcast_to(OB[h, pl.ds(o, 1), :], (GRID_W, 128))
                two = jnp.broadcast_to(OB[h, pl.ds(o + 1, 1), :], (GRID_W, 128))
                one = pltpu.roll(one, 113, 1, stride=1, stride_axis=0)
                two = pltpu.roll(two, 49, 1, stride=1, stride_axis=0)
                T2[h, o] = jnp.where(valid, jnp.where(lane < GRID_W, one, two), NEG)

    with jax.named_scope("ms_wait"):
        @pl.loop(1, 8)
        def _(k):
            ms_copy((tp + k) % 8, k).wait_recv()

    for t in range(8):
        cols = slice(t * WIDE, (t + 1) * WIDE)
        block = MS[t]
        MOD[0:1, cols] = block[0:1]
        MOD[1:2, cols] = norm_gain[:, cols] * (1.0 + block[1:2])
        MOD[2:3, cols] = block[2:3]

    loads[7].wait()

    lo = jnp.where(sp == 0, 0, -4)
    hi = jnp.where(sp == 15, 16, 20)
    factor = HEAD**-0.5 * LOG2E
    STRIPS = range(0, SHARD, 16)

    def piece_of(s, j):
        r, n, side = s // 2, s % 2, j % 2
        dx = jnp.where(r == 0, 0, jnp.where(r == 3, 2, 3 - 2 * side))
        core = c if j < 2 else mate
        shift = jnp.where(r == 2, 2, 0)
        later = n + shift if side == 0 else 3 - n - shift
        return (((x + dx) % 4) * 2 + core) * 4 + jnp.where(r == 0, 2 * n + side, later)

    def full(v):
        return jnp.broadcast_to(v, (16, 128))

    def tiles(v):
        return [v[:, n * 128 : (n + 1) * 128] for n in range(v.shape[1] // 128)]

    def tree(parts, op):
        while len(parts) > 1:
            parts = [op(p, q) for p, q in zip(parts[::2], parts[1::2])] + parts[len(parts) & ~1 :]
        return parts[0]

    def spread(ref, rows, new):
        ref[rows, 0:HEAD] = new[:, 0:HEAD]
        ref[rows, HEAD : 2 * HEAD] = jnp.ones_like(new[:, 0:HEAD])
        ref[rows, 2 * HEAD :] = new[:, HEAD:]

    def split(h, both):
        out_part, sums = both[:, 0:HEAD], both[:, HEAD:]
        return (out_part, sums) if h == 0 else (sums, out_part)

    def norm_rows(piece, at):
        for i in range(3):
            v = G[piece, i * 16 : i * 16 + 16, :].astype(F32)
            L[at + i * 16 : at + i * 16 + 16, :] = full(inv_rms(v))
        for i in range(3):
            rows = slice(at + i * 16, at + i * 16 + 16)
            inv = L[rows, :]
            for n in range(D // 128):
                cols = slice(n * 128, (n + 1) * 128)
                v = G[piece, i * 16 : i * 16 + 16, cols].astype(F32)
                NRM[rows, cols] = (v * inv * MOD[1:2, cols] + MOD[0:1, cols]).astype(BF16)

    def head_rows(piece, at, slot):
        for i in range(3):
            rows = slice(at + i * 16, at + i * 16 + 16)
            q_rows = pl.ds(pl.multiple_of(piece * QUART + i * 16, 16), 16)
            k_rows = pl.ds(pl.multiple_of(piece * QUART + i * 16 + PAD, 16), 16)
            for h in range(2):
                a, b = h * HEAD, (h + 1) * HEAD
                part = R[rows, a:b]
                part = (part * inv_rms(part) * qg).astype(BF16)
                Q[q_rows, a:b] = part
                QN[slot, rows, a:b] = part
                part = R[rows, WIDE + a : WIDE + b]
                KV[k_rows, a:b] = (part * inv_rms(part) * kg).astype(BF16)
            new = R[rows, 2 * WIDE :].astype(BF16)
            KV[k_rows, WIDE:] = new
            spread(VA, k_rows, new)

    def halo_copy(piece, k):
        src = pl.multiple_of(piece * QUART + PAD, 16)
        low = k < 6
        dst = pl.multiple_of(k * QUART + jnp.where(low, PAD + TOK, -PAD), 16)
        return pltpu.make_async_remote_copy(
            src_ref=KV.at[pl.ds(src, QUART)], dst_ref=KV.at[pl.ds(dst, QUART)],
            send_sem=halo_send.at[k], recv_sem=halo_recv.at[k],
            device_id=sp_dev((sp + jnp.where(low, 15, 1)) % 16), device_id_type=MESH,
        )

    def context_part(s, slot):
        for h in range(2):
            a, b = h * HEAD, (h + 1) * HEAD
            S[h] = dot_nt(QN[slot, :, a:b], CKV[:, a:b])
        for h in range(2):
            a, b = h * HEAD, (h + 1) * HEAD
            cb = context_bias[h] * LOG2E
            pieces = [piece_of(s, j) for j in range(4)]

            def place(at):
                return pl.ds(pl.multiple_of(pieces[at // QUART] * QUART + at % QUART, 16), 16)

            for at in STRIPS:
                top = tree(tiles(S[h, at : at + 16, :]), jnp.maximum) * factor + cb
                MC[h, place(at), :] = full(jnp.max(top, axis=1, keepdims=True))
            for at in STRIPS:
                top = MC[h, place(at), :] - cb
                for n in range(CTX // 128):
                    cols = slice(n * 128, (n + 1) * 128)
                    PR[h, at : at + 16, cols] = jnp.exp2(
                        S[h, at : at + 16, cols] * factor - top
                    ).astype(BF16)
            acc, sums = split(h, dot(PR[h], CVA[:, a : a + WIDE]))
            for j in range(4):
                rows = pl.ds(pl.multiple_of(pieces[j] * QUART, 16), QUART)
                ACC[rows, a:b] = acc[j * QUART : (j + 1) * QUART]
                LC[h, rows, :] = sums[j * QUART : (j + 1) * QUART]

    def window_part(t):
        base = pl.multiple_of(t * SHARD, SHARD)
        keys, offsets = [], []
        for i in range(3):
            row = t * 3 + i
            start = jnp.minimum(jnp.maximum(row - 4, lo), hi)
            keys.append(pl.ds(pl.multiple_of(start * GRID_W + PAD, 32), 512))
            offsets.append(start - row + 7)
        for h in range(2):
            a, b = h * HEAD, (h + 1) * HEAD
            for i in range(3):
                SW[h, i * 64 : (i + 1) * 64, :] = dot_nt(
                    Q[pl.ds(base + i * 64, 64), a:b], KV[keys[i], a:b]
                )
        for h in range(2):
            a, b = h * HEAD, (h + 1) * HEAD

            def scores(at):
                i, sub = at // 64, slice(at % 64, at % 64 + 16)
                return [
                    SW[h, at : at + 16, n * 128 : (n + 1) * 128] * factor
                    + T2[h, offsets[i] + 2 * n, sub, :]
                    for n in range(4)
                ]

            for at in STRIPS:
                top = jnp.max(tree(scores(at), jnp.maximum), axis=1, keepdims=True)
                M[h, at : at + 16, :] = jnp.maximum(full(top), MC[h, pl.ds(base + at, 16), :])
            for at in STRIPS:
                top = M[h, at : at + 16, :]
                for n, one in enumerate(scores(at)):
                    PW[h, at : at + 16, n * 128 : (n + 1) * 128] = jnp.exp2(one - top).astype(BF16)
            for i in range(3):
                part, rows = slice(i * 64, (i + 1) * 64), pl.ds(base + i * 64, 64)
                new, sums = split(h, dot(PW[h, part, :], VA[keys[i], a : a + WIDE]))
                keep = jnp.exp2(MC[h, rows, :] - M[h, part, :])
                norm = 1.0 / (sums + LC[h, rows, :] * keep)
                ATT[t, part, a:b] = ((new + ACC[rows, a:b] * keep) * norm).astype(BF16)

    @pl.loop(0, 8)
    def _(s):
        r, n = s // 2, s % 2
        pieces = [piece_of(s, j) for j in range(4)]

        for j in range(4):
            if j >= 2:
                with jax.named_scope("mate_wait"):
                    ag_copy(pieces[j], 0, to_right).wait_recv()
            norm_rows(pieces[j], j * QUART)

        with jax.named_scope("qkv"):
            for k, w in enumerate((WQ, WK, WV)):
                R[:, k * WIDE : (k + 1) * WIDE] = dot(NRM[...], w[...])
        for j in range(4):
            head_rows(pieces[j], j * QUART, n)
        for j in range(4):
            piece = pieces[j]

            @pl.when((piece < 6) | (piece >= 26))
            def _():
                halo_copy(piece, jnp.where(piece < 6, piece, piece - 20)).start()

        @pl.when((s > 0) & (s < 7))
        def _():
            for j in range(2):
                piece = piece_of(s + 1, j)
                with jax.named_scope("ring_wait"):
                    ag_copy(piece, 0, to_right).wait_recv()
                ag_copy(piece, 8 + 2 * (s + 1) + j, to_mate).start()

                @pl.when((s + 1) // 2 == 1)
                def _():
                    ag_copy(piece, 24 + 2 * j + (s + 1) % 2, to_right if j == 0 else to_left).start()

        @pl.when(s == 1)
        def _():
            with jax.named_scope("ctx_wait"):
                @pl.loop(1, 16)
                def _(k):
                    cx_copy((sp + k) % 16, k).wait_recv()

            for e in range(0, CTX, 128):
                spread(CVA, slice(e, e + 128), CKV[e : e + 128, WIDE:])

        with jax.named_scope("ctx_part"):
            @pl.loop(jnp.where(s < 2, 0, s), jnp.where(s == 0, 0, s + 1))
            def _(e):
                context_part(e, e % 2)

    def aa_copy(t, src, k):
        half = pl.ds(pl.multiple_of(src % 2 * WIDE, WIDE), WIDE)
        return pltpu.make_async_remote_copy(
            src_ref=ATT.at[t], dst_ref=RX.at[src // 2, :, half], send_sem=aa_send.at[k],
            recv_sem=aa_recv.at[src], device_id=tp_dev(t), device_id_type=MESH,
        )

    first_low = jnp.where(tp == 0, 1, 0)
    near = jnp.where(x < 2, 1, 3)

    with jax.named_scope("window"):
        @pl.loop(0, 8)
        def _(k):
            far = (k < 4) & (k % 2 == 0)
            dx = jnp.where(k >= 6, 0, jnp.where(far, 2, jnp.where(k < 4, near, 4 - near)))
            core = jnp.where(k == 6, mate, jnp.where(k == 7, c, jnp.where(k < 4, k // 2, k - 4)))
            t = (x + dx) % 4 * 2 + core

            @pl.when(t == first_low)
            def _():
                with jax.named_scope("halo_low"):
                    for n in range(6, 12):
                        halo_copy(n + 20, n).wait_recv()
                spread(VA, slice(0, PAD), KV[0:PAD, WIDE:])

            @pl.when(t == 7)
            def _():
                with jax.named_scope("halo_high"):
                    for n in range(6):
                        halo_copy(n, n).wait_recv()
                spread(VA, slice(PAD + TOK, 2 * PAD + TOK), KV[PAD + TOK :, WIDE:])

            window_part(t)

            @pl.when(k < 7)
            def _():
                aa_copy(t, tp, k).start()

    own_half = pl.ds(pl.multiple_of(c * WIDE, WIDE), WIDE)
    RX[x, :, own_half] = ATT[tp]
    loads[8].wait()

    for g, dx in enumerate((3, 0, 1, 2)):
        chip = (x + dx) % 4
        with jax.named_scope("aa_wait"):
            if g != 1:
                aa_copy(tp, chip * 2, 0).wait_recv()
                aa_copy(tp, chip * 2 + 1, 0).wait_recv()
            else:
                aa_copy(tp, x * 2 + mate, 0).wait_recv()
        with jax.named_scope("project"):
            for n in range(8):
                cols = slice(n * WIDE, (n + 1) * WIDE)
                rows = pl.ds(pl.multiple_of(chip * 2 * WIDE, 2 * WIDE), 2 * WIDE)
                part = dot(RX[chip], WO[rows, cols])
                if g > 0:
                    part = part + PA[:, cols]
                if g < 3:
                    PA[:, cols] = part
                else:
                    for s in range(4):
                        some = slice(s * QUART, (s + 1) * QUART)
                        mine = G[own + s, :, cols].astype(F32)
                        out[some, cols] = (mine + MOD[2:3, cols] * part[some]).astype(BF16)

    with jax.named_scope("drain"):
        for slot in range(28):
            ag_copy(own, slot, to_mate).wait_send()

        @pl.loop(1, 16)
        def _(k):
            mp_copy(k).wait_send()
            cx_copy(sp, k).wait_send()

        @pl.loop(1, 8)
        def _(k):
            ms_copy(tp, k).wait_send()
            aa_copy(tp, tp, k - 1).wait_send()

        for n in range(12):
            halo_copy(0, n).wait_send()


def shards(
    resid, cond, mod_shift, mod_scale, mod_gate, norm_gain, context, w_query, w_key, w_value,
    query_gain, key_gain, offset_bias, context_bias, w_out,
):
    vmem = pl.BlockSpec(memory_space=pltpu.VMEM)
    smem = pl.BlockSpec(memory_space=pltpu.SMEM)
    hbm = pl.BlockSpec(memory_space=pl.ANY)
    dma = pltpu.SemaphoreType.DMA
    scratch = [
        pltpu.VMEM((32, QUART, D), BF16),
        pltpu.VMEM((D, WIDE), BF16),
        pltpu.VMEM((D, WIDE), BF16),
        pltpu.VMEM((D, WIDE), BF16),
        pltpu.VMEM((D, D), BF16),
        pltpu.VMEM((64, D), BF16),
        pltpu.VMEM((SHARD, D), BF16),
        pltpu.VMEM((SHARD, 3 * WIDE), F32),
        pltpu.VMEM((TOK, WIDE), BF16),
        pltpu.VMEM((TOK + 2 * PAD, 2 * WIDE), BF16),
        pltpu.VMEM((CTX, 2 * WIDE), BF16),
        pltpu.VMEM((16, 8, WIDE), F32),
        pltpu.VMEM((8, 8, WIDE), F32),
        pltpu.VMEM((8, WIDE), F32),
        pltpu.VMEM((8, D), F32),
        pltpu.VMEM((2, 16, 128), F32),
        pltpu.VMEM((2, 14, GRID_W, 128), F32),
        pltpu.VMEM((2, SHARD, CTX), F32),
        pltpu.VMEM((2, SHARD, CTX), BF16),
        pltpu.VMEM((2, SHARD, 512), F32),
        pltpu.VMEM((2, SHARD, 512), BF16),
        pltpu.VMEM((TOK + 2 * PAD, 3 * HEAD), BF16),
        pltpu.VMEM((CTX, 3 * HEAD), BF16),
        pltpu.VMEM((2, SHARD, WIDE), BF16),
        pltpu.VMEM((TOK, WIDE), F32),
        pltpu.VMEM((2, TOK, HEAD), F32),
        pltpu.VMEM((2, TOK, HEAD), F32),
        pltpu.VMEM((2, SHARD, HEAD), F32),
        pltpu.VMEM((SHARD, HEAD), F32),
        pltpu.VMEM((SHARD, D), F32),
        pltpu.VMEM((8, SHARD, WIDE), BF16),
        pltpu.VMEM((4, SHARD, 2 * WIDE), BF16),
        dma((9,)), dma((28,)), dma((32,)), dma((16,)), dma((16,)), dma((8,)), dma((8,)),
        dma((16,)), dma((16,)), dma((12,)), dma((12,)), dma((8,)), dma((8,)),
    ]
    return pl.pallas_call(
        kernel,
        out_shape=jax.ShapeDtypeStruct((SHARD, D), BF16),
        in_specs=[hbm, vmem, vmem, vmem, vmem, vmem, hbm, hbm, hbm, hbm, vmem, vmem, vmem, smem, hbm],
        out_specs=vmem,
        scratch_shapes=scratch,
        compiler_params=pltpu.CompilerParams(
            collective_id=0, has_side_effects=True, vmem_limit_bytes=60 * 1024 * 1024
        ),
    )(
        resid, cond.reshape(1, -1), mod_shift, mod_scale, mod_gate, norm_gain.reshape(1, -1),
        context, w_query, w_key, w_value, query_gain.reshape(1, -1), key_gain.reshape(1, -1),
        jnp.transpose(offset_bias, (1, 0, 2)), context_bias, w_out,
    )


def solution(mesh):
    grid = Mesh(mesh.devices.reshape(4, 4, 4, 2), ("z", "y", "x", "c"))
    sp, tp, both = ("z", "y"), ("x", "c"), ("z", "y", "x", "c")
    placed = (
        P(both, None), P(sp), P(sp, tp), P(sp, tp), P(sp, tp), P(), P(sp, None),
        P(None, tp), P(None, tp), P(None, tp), P(), P(), P(tp, None, None), P(tp), P(),
    )
    return jax.shard_map(
        shards, mesh=grid, in_specs=placed, out_specs=P(both, None), check_vma=False
    )
```

```python
import functools

import jax
import jax.numpy as jnp
from jax import lax
from jax.experimental import pallas as pl
from jax.experimental.pallas import tpu as pltpu
from jax.sharding import Mesh
from jax.sharding import PartitionSpec as P

MESH = pl.DeviceIdType.MESH
BF16, F32 = jnp.bfloat16, jnp.float32
EPS = 1e-06
LOG2E = 1.4426950408889634
HEAD = 128
GRID_W = 64
D = 2048
CTX = 1024
ROWS_DEV = 24
TOK = 1536
SHARD = 192
PAD = 288
HALF = 96
QUART = 48
WIDE = 256
NEG = -1e30
NT = (((1,), (1,)), ((), ()))


def dot_nt(a, b):
    return lax.dot_general(a, b, NT, preferred_element_type=F32)


def dot(a, b):
    return jnp.dot(a, b, preferred_element_type=F32)


def inv_rms(v):
    return lax.rsqrt(jnp.mean(v * v, axis=-1, keepdims=True) + EPS)


def kernel(
    resid, cond, mod_shift, mod_scale, mod_gate, norm_gain, context, w_query, w_key, w_value,
    query_gain, key_gain, offset_bias, context_bias, w_out, out,
    G, WQ, WK, WV, WO, CX, NRM, R, Q, KV, CK, CV, MP, MS, MSUM, MOD, OB, T2, S, PR, SW, PW, VA, CVA, QN, ACC, MC, LC, M, L, PA, RL, ATT, RX,
    load_sem, ag_send, ag_recv, mp_send, mp_recv, ms_send, ms_recv, cx_send, cx_recv,
    halo_send, halo_recv, aa_send, aa_recv, rl_send, rl_recv,
):
    z, y, x, c = (lax.axis_index(a) for a in ("z", "y", "x", "c"))
    sp, tp = z * 4 + y, x * 2 + c
    right, left, opp, mate = (x + 1) % 4, (x + 3) % 4, (x + 2) % 4, 1 - c

    def sp_dev(s):
        return (s // 4, s % 4, x, c)

    def tp_dev(t):
        return (z, y, t // 2, t % 2)

    with jax.named_scope("entry"):
        loads = [
            pltpu.make_async_copy(
                resid.at[pl.ds(n * QUART, QUART)], G.at[tp * 4 + n], load_sem.at[n]
            )
            for n in range(4)
        ] + [
            pltpu.make_async_copy(context, CX, load_sem.at[4]),
            pltpu.make_async_copy(w_key, WK, load_sem.at[5]),
            pltpu.make_async_copy(w_value, WV, load_sem.at[6]),
            pltpu.make_async_copy(w_query, WQ, load_sem.at[7]),
            pltpu.make_async_copy(w_out, WO, load_sem.at[8]),
        ]
        for one in loads:
            one.start()

        barrier = pltpu.get_barrier_semaphore()

        @pl.loop(1, 8)
        def _(k):
            pl.semaphore_signal(barrier, inc=1, device_id=tp_dev((tp + k) % 8), device_id_type=MESH)

        @pl.loop(1, 16)
        def _(k):
            pl.semaphore_signal(barrier, inc=1, device_id=sp_dev((sp + k) % 16), device_id_type=MESH)

        cf = cond[...].astype(F32)
        lifted = jnp.broadcast_to(cf / (1.0 + jnp.exp(-cf)), (16, 128)).astype(BF16)
        rows8 = lax.broadcasted_iota(jnp.int32, (8, WIDE), 0)
        p_shift = dot(lifted, mod_shift[...])[0:8]
        p_scale = dot(lifted, mod_scale[...])[0:8]
        p_gate = dot(lifted, mod_gate[...])[0:8]
        MP[sp] = jnp.where(rows8 == 0, p_shift, jnp.where(rows8 == 1, p_scale, p_gate))

        pl.semaphore_wait(barrier, 22)

    def ag_copy(chunk, slot, device):
        return pltpu.make_async_remote_copy(
            src_ref=G.at[chunk], dst_ref=G.at[chunk], send_sem=ag_send.at[slot],
            recv_sem=ag_recv.at[chunk], device_id=device, device_id_type=MESH,
        )

    to_right, to_left, to_mate = (z, y, right, c), (z, y, left, c), (z, y, x, mate)
    to_right, to_left, to_mate = (z, y, right, c), (z, y, left, c), (z, y, x, mate)
    own = tp * 4
    for n in range(4):
        loads[n].wait()
    ag_copy(own, 0, to_right).start()
    ag_copy(own + 3, 4, to_left).start()
    for n in range(4):
        ag_copy(own + n, 8 + n, to_mate).start()

    def mp_copy(k):
        return pltpu.make_async_remote_copy(
            src_ref=MP.at[sp], dst_ref=MP.at[sp], send_sem=mp_send.at[k],
            recv_sem=mp_recv.at[sp], device_id=sp_dev((sp + k) % 16), device_id_type=MESH,
        )

    def mp_wait(k):
        s = (sp + k) % 16
        return pltpu.make_async_remote_copy(
            src_ref=MP.at[s], dst_ref=MP.at[s], send_sem=mp_send.at[k],
            recv_sem=mp_recv.at[s], device_id=sp_dev(s), device_id_type=MESH,
        )

    @pl.loop(1, 16)
    def _(k):
        mp_copy(k).start()

    loads[4].wait()

    @pl.loop(0, 4)
    def _(i):
        rows = pl.ds(pl.multiple_of(i * 16, 16), 16)
        v = CX[rows, :].astype(F32)
        NRM[rows, :] = (v * inv_rms(v) * norm_gain[...]).astype(BF16)

    loads[5].wait()
    loads[6].wait()
    kg, qg = key_gain[...], query_gain[...]
    ck = dot(NRM[0:64, :], WK[...])
    cv = dot(NRM[0:64, :], WV[...])
    key_rows = pl.ds(pl.multiple_of(sp * 64, 64), 64)
    for h in range(2):
        part = ck[:, h * HEAD : (h + 1) * HEAD]
        CK[key_rows, h * HEAD : (h + 1) * HEAD] = (part * inv_rms(part) * kg).astype(BF16)
    CV[pl.ds(pl.multiple_of((y * 4 + z) * 64, 64), 64), :] = cv.astype(BF16)

    def cx_copy(leg, source, o):
        along_y = leg in (0, 3)
        ref, count = (CK, CV, CK, CV)[leg], 64 if leg < 2 else 256
        at = (source, source, source, source)[leg] * count + (0 if leg > 1 else (z, y)[leg] * 256)
        rows = pl.ds(pl.multiple_of(at, 64), count)
        return pltpu.make_async_remote_copy(
            src_ref=ref.at[rows], dst_ref=ref.at[rows], send_sem=cx_send.at[leg * 4 + o],
            recv_sem=cx_recv.at[leg * 4 + source],
            device_id=(z, (y + o) % 4, x, c) if along_y else ((z + o) % 4, y, x, c),
            device_id_type=MESH,
        )

    def cx_start(leg):
        for o in (2, 1, 3):
            cx_copy(leg, y if leg in (0, 3) else z, o).start()

    def cx_wait(leg):
        for o in (1, 3, 2):
            cx_copy(leg, ((y if leg in (0, 3) else z) + o) % 4, o).wait_recv()

    cx_start(0)
    cx_start(1)

    with jax.named_scope("mp_wait"):
        @pl.loop(1, 16)
        def _(k):
            mp_wait(k).wait_recv()

    total = MP[0]
    for s in range(1, 16):
        total = total + MP[s]
    MS[tp] = total

    def ms_copy(t, k):
        return pltpu.make_async_remote_copy(
            src_ref=MS.at[t], dst_ref=MS.at[t], send_sem=ms_send.at[k],
            recv_sem=ms_recv.at[t], device_id=tp_dev((tp + k) % 8), device_id_type=MESH,
        )

    @pl.loop(1, 8)
    def _(k):
        ms_copy(tp, k).start()

    for n in range(1, 4):
        ag_copy(own + n, n, to_right).start()
        ag_copy(own + 3 - n, 4 + n, to_left).start()

    with jax.named_scope("ctx_turn"):
        for leg in range(2):
            cx_wait(leg)
            cx_start(leg + 2)

    with jax.named_scope("bias"):
        OB[...] = jnp.zeros_like(OB)
        for h in range(2):
            OB[h, 0:15, 0:31] = offset_bias[:, h, :] * LOG2E
        col = lax.broadcasted_iota(jnp.int32, (GRID_W, 128), 0)
        lane = lax.broadcasted_iota(jnp.int32, (GRID_W, 128), 1)
        key_col = lane % GRID_W
        begin = jnp.clip(col - 8, 0, GRID_W - 16)
        valid = (key_col >= begin) & (key_col < begin + 16)
        for h in range(2):

            @pl.loop(0, 14)
            def _(o):
                one = jnp.broadcast_to(OB[h, pl.ds(o, 1), :], (GRID_W, 128))
                two = jnp.broadcast_to(OB[h, pl.ds(o + 1, 1), :], (GRID_W, 128))
                one = pltpu.roll(one, 113, 1, stride=1, stride_axis=0)
                two = pltpu.roll(two, 49, 1, stride=1, stride_axis=0)
                T2[h, o] = jnp.where(valid, jnp.where(lane < GRID_W, one, two), NEG)

    with jax.named_scope("ms_wait"):
        @pl.loop(1, 8)
        def _(k):
            ms_copy((tp + k) % 8, k).wait_recv()

    for t in range(8):
        cols = slice(t * WIDE, (t + 1) * WIDE)
        block = MS[t]
        MOD[0:1, cols] = block[0:1]
        MOD[1:2, cols] = norm_gain[:, cols] * (1.0 + block[1:2])
        MOD[2:3, cols] = block[2:3]

    loads[7].wait()

    lo = jnp.where(sp == 0, 0, -4)
    hi = jnp.where(sp == 15, 16, 20)
    factor = HEAD**-0.5 * LOG2E
    STRIPS = range(0, SHARD, 16)

    def piece_of(s, j):
        r, n, side = s // 2, s % 2, j % 2
        dx = jnp.where(r == 0, 0, jnp.where(r == 3, 2, 3 - 2 * side))
        core = c if j < 2 else mate
        shift = jnp.where(r == 2, 2, 0)
        later = n + shift if side == 0 else 3 - n - shift
        return (((x + dx) % 4) * 2 + core) * 4 + jnp.where(r == 0, 2 * n + side, later)

    def full(v):
        return jnp.broadcast_to(v, (16, 128))

    def tiles(v):
        return [v[:, n * 128 : (n + 1) * 128] for n in range(v.shape[1] // 128)]

    def tree(parts, op):
        while len(parts) > 1:
            parts = [op(p, q) for p, q in zip(parts[::2], parts[1::2])] + parts[len(parts) & ~1 :]
        return parts[0]

    def spread(ref, rows, new):
        ref[rows, 0:HEAD] = new[:, 0:HEAD]
        ref[rows, HEAD : 2 * HEAD] = jnp.ones_like(new[:, 0:HEAD])
        ref[rows, 2 * HEAD :] = new[:, HEAD:]

    def split(h, both):
        out_part, sums = both[:, 0:HEAD], both[:, HEAD:]
        return (out_part, sums) if h == 0 else (sums, out_part)

    def norm_rows(piece, at):
        for i in range(3):
            v = G[piece, i * 16 : i * 16 + 16, :].astype(F32)
            L[at + i * 16 : at + i * 16 + 16, :] = full(inv_rms(v))
        for i in range(3):
            rows = slice(at + i * 16, at + i * 16 + 16)
            inv = L[rows, :]
            for n in range(D // 128):
                cols = slice(n * 128, (n + 1) * 128)
                v = G[piece, i * 16 : i * 16 + 16, cols].astype(F32)
                NRM[rows, cols] = (v * inv * MOD[1:2, cols] + MOD[0:1, cols]).astype(BF16)

    def head_rows(piece, at, slot):
        for i in range(3):
            rows = slice(at + i * 16, at + i * 16 + 16)
            q_rows = pl.ds(pl.multiple_of(piece * QUART + i * 16, 16), 16)
            k_rows = pl.ds(pl.multiple_of(piece * QUART + i * 16 + PAD, 16), 16)
            for h in range(2):
                a, b = h * HEAD, (h + 1) * HEAD
                part = R[rows, a:b]
                part = (part * inv_rms(part) * qg).astype(BF16)
                Q[q_rows, a:b] = part
                QN[slot, rows, a:b] = part
                part = R[rows, WIDE + a : WIDE + b]
                KV[k_rows, a:b] = (part * inv_rms(part) * kg).astype(BF16)
            new = R[rows, 2 * WIDE :].astype(BF16)
            KV[k_rows, WIDE:] = new
            spread(VA, k_rows, new)

    def halo_copy(piece, k):
        src = pl.multiple_of(piece * QUART + PAD, 16)
        low = k < 6
        dst = pl.multiple_of(k * QUART + jnp.where(low, PAD + TOK, -PAD), 16)
        return pltpu.make_async_remote_copy(
            src_ref=KV.at[pl.ds(src, QUART)], dst_ref=KV.at[pl.ds(dst, QUART)],
            send_sem=halo_send.at[k], recv_sem=halo_recv.at[k],
            device_id=sp_dev((sp + jnp.where(low, 15, 1)) % 16), device_id_type=MESH,
        )

    def context_head(s, h):
        pieces = [piece_of(s, j) for j in range(4)]
        a, b = h * HEAD, (h + 1) * HEAD
        cb = context_bias[h] * LOG2E

        def place(at):
            return pl.ds(pl.multiple_of(pieces[at // QUART] * QUART + at % QUART, 16), 16)

        S[h] = dot_nt(QN[s % 4, :, a:b], CK[:, a:b])
        for at in STRIPS:
            top = tree(tiles(S[h, at : at + 16, :]), jnp.maximum) * factor + cb
            MC[h, place(at), :] = full(jnp.max(top, axis=1, keepdims=True))
        for at in STRIPS:
            top = MC[h, place(at), :] - cb
            for n in range(CTX // 128):
                cols = slice(n * 128, (n + 1) * 128)
                PR[h, at : at + 16, cols] = jnp.exp2(
                    S[h, at : at + 16, cols] * factor - top
                ).astype(BF16)
        acc, sums = split(h, dot(PR[h], CVA[:, a : a + WIDE]))
        for j in range(4):
            rows = pl.ds(pl.multiple_of(pieces[j] * QUART, 16), QUART)
            ACC[rows, a:b] = acc[j * QUART : (j + 1) * QUART]
            LC[h, rows, :] = sums[j * QUART : (j + 1) * QUART]

    def window_part(t):
        base = pl.multiple_of(t * SHARD, SHARD)
        keys, offsets = [], []
        for i in range(3):
            row = t * 3 + i
            start = jnp.minimum(jnp.maximum(row - 4, lo), hi)
            keys.append(pl.ds(pl.multiple_of(start * GRID_W + PAD, 32), 512))
            offsets.append(start - row + 7)
        for h in range(2):
            a, b = h * HEAD, (h + 1) * HEAD
            for i in range(3):
                SW[h, i * 64 : (i + 1) * 64, :] = dot_nt(
                    Q[pl.ds(base + i * 64, 64), a:b], KV[keys[i], a:b]
                )
        for h in range(2):
            a, b = h * HEAD, (h + 1) * HEAD

            def scores(at):
                i, sub = at // 64, slice(at % 64, at % 64 + 16)
                return [
                    SW[h, at : at + 16, n * 128 : (n + 1) * 128] * factor
                    + T2[h, offsets[i] + 2 * n, sub, :]
                    for n in range(4)
                ]

            for at in STRIPS:
                top = jnp.max(tree(scores(at), jnp.maximum), axis=1, keepdims=True)
                M[h, at : at + 16, :] = jnp.maximum(full(top), MC[h, pl.ds(base + at, 16), :])
            for at in STRIPS:
                top = M[h, at : at + 16, :]
                for n, one in enumerate(scores(at)):
                    PW[h, at : at + 16, n * 128 : (n + 1) * 128] = jnp.exp2(one - top).astype(BF16)
            for i in range(3):
                part, rows = slice(i * 64, (i + 1) * 64), pl.ds(base + i * 64, 64)
                new, sums = split(h, dot(PW[h, part, :], VA[keys[i], a : a + WIDE]))
                keep = jnp.exp2(MC[h, rows, :] - M[h, part, :])
                norm = 1.0 / (sums + LC[h, rows, :] * keep)
                ATT[t, part, a:b] = ((new + ACC[rows, a:b] * keep) * norm).astype(BF16)

    def aa_copy(t, src, k):
        half = pl.ds(pl.multiple_of(src % 2 * WIDE, WIDE), WIDE)
        return pltpu.make_async_remote_copy(
            src_ref=ATT.at[t], dst_ref=RX.at[src // 2, :, half], send_sem=aa_send.at[k],
            recv_sem=aa_recv.at[src], device_id=tp_dev(t), device_id_type=MESH,
        )

    onward = jnp.where(c == 0, right, left)
    behind = jnp.where(c == 0, left, right)

    def relay_in(i):
        return pltpu.make_async_remote_copy(
            src_ref=ATT.at[opp * 2 + i], dst_ref=RL.at[i], send_sem=rl_send.at[i],
            recv_sem=rl_recv.at[i], device_id=(z, y, onward, c), device_id_type=MESH,
        )

    def relay_out(i):
        half = pl.ds(pl.multiple_of(c * WIDE, WIDE), WIDE)
        return pltpu.make_async_remote_copy(
            src_ref=RL.at[i], dst_ref=RX.at[behind, :, half], send_sem=rl_send.at[2 + i],
            recv_sem=aa_recv.at[behind * 2 + c], device_id=(z, y, onward, i), device_id_type=MESH,
        )

    first_low = jnp.where(tp == 1, 0, jnp.where(tp == 0, 1, 0))
    near = jnp.where(x < 2, 1, 3)

    def window(t):
        @pl.when(t == first_low)
        def _():
            with jax.named_scope("halo_low"):
                for n in range(6, 12):
                    halo_copy(n + 20, n).wait_recv()
            spread(VA, slice(0, PAD), KV[0:PAD, WIDE:])

        @pl.when(t == 7)
        def _():
            with jax.named_scope("halo_high"):
                for n in range(6):
                    halo_copy(n, n).wait_recv()
            spread(VA, slice(PAD + TOK, 2 * PAD + TOK), KV[PAD + TOK :, WIDE:])

        window_part(t)

    def norm_project(s):
        pieces = [piece_of(s, j) for j in range(4)]
        with jax.named_scope("mate_wait"):
            for j in (2, 3):
                ag_copy(pieces[j], 0, to_right).wait_recv()
        for j in range(4):
            norm_rows(pieces[j], j * QUART)
        for k, w in enumerate((WQ, WK, WV)):
            R[:, k * WIDE : (k + 1) * WIDE] = dot(NRM[...], w[...])

    def take_next(s):
        for j in range(2):
            piece = piece_of(s, j)
            with jax.named_scope("ring_wait"):
                ag_copy(piece, 0, to_right).wait_recv()
            ag_copy(piece, 8 + 2 * s + j, to_mate).start()

            @pl.when(s // 2 == 1)
            def _():
                ag_copy(piece, 24 + 2 * j + s % 2, to_right if j == 0 else to_left).start()

    def heads(s):
        for j in range(4):
            head_rows(piece_of(s, j), j * QUART, s % 4)

    def send_halo(s):
        for j in range(4):
            piece = piece_of(s, j)

            @pl.when((piece < 6) | (piece >= 26))
            def _():
                halo_copy(piece, jnp.where(piece < 6, piece, piece - 20)).start()

    @pl.loop(0, 3)
    def _(s):
        @pl.when(s > 0)
        def _():
            take_next(s + 1)

        with jax.named_scope("first_half"):
            norm_project(s)
        with jax.named_scope("second_half"):
            heads(s)
        send_halo(s)

    with jax.named_scope("ctx_wait"):
        cx_wait(2)
        cx_wait(3)

    for e in range(16):
        spread(CVA, slice(e * 64, e * 64 + 64), CV[pl.ds((e % 4 * 4 + e // 4) * 64, 64), :])
    with jax.named_scope("ctx01"):
        @pl.loop(0, 2)
        def _(e):
            context_head(e, 0)
            context_head(e, 1)

    @pl.loop(3, 6)
    def _(s):
        take_next(s + 1)
        with jax.named_scope("first_half"):
            norm_project(s)
            context_head(s - 1, 0)
        with jax.named_scope("second_half"):
            heads(s)
            context_head(s - 1, 1)
        send_halo(s)

    s6, s7 = tp * 0 + 6, tp * 0 + 7
    with jax.named_scope("first_half"):
        norm_project(s6)
        context_head(5, 0)
    take_next(s7)
    with jax.named_scope("second_half"):
        heads(s6)
        context_head(5, 1)
        context_head(6, 0)
    send_halo(s6)
    with jax.named_scope("first_half"):
        norm_project(s7)
    with jax.named_scope("second_half"):
        heads(s7)
    send_halo(s7)
    with jax.named_scope("ctx7"):
        context_head(6, 1)
        context_head(7, 0)
        context_head(7, 1)

    with jax.named_scope("window"):
        @pl.loop(0, 8)
        def _(k):
            home = (k == 4) | (k == 5)
            middle = (x == 1) | (x == 2)
            side = jnp.where(middle, jnp.where(k < 4, near, 4 - near), 1 + k % 2 * 2)
            dx = jnp.where(home, 0, jnp.where(k < 2, 2, side))
            core = jnp.where(home, (mate + k) % 2, k % 2)
            core = jnp.where(middle | (k < 6) & (home | (k < 2)), core, k // 4)
            t = (x + dx) % 4 * 2 + core

            @pl.when((k == 5) | (k == 6))
            def _():
                with jax.named_scope("relay_wait"):
                    relay_in(k - 5).wait_recv()
                relay_out(k - 5).start()

            window(t)

            @pl.when(k < 2)
            def _():
                relay_in(k).start()

            @pl.when((k >= 2) & (k != 5))
            def _():
                aa_copy(t, tp, jnp.where(k < 5, k, k - 1)).start()

    own_half = pl.ds(pl.multiple_of(c * WIDE, WIDE), WIDE)
    RX[x, :, own_half] = ATT[tp]
    loads[8].wait()

    odd = x % 2
    for g, dx in enumerate((3 - 2 * odd, 0, 2, 1 + 2 * odd)):
        chip = (x + dx) % 4
        with jax.named_scope("aa_wait"):
            if g != 1:
                aa_copy(tp, chip * 2, 0).wait_recv()
                aa_copy(tp, chip * 2 + 1, 0).wait_recv()
            else:
                aa_copy(tp, x * 2 + mate, 0).wait_recv()
        with jax.named_scope("project"):
            for n in range(8):
                cols = slice(n * WIDE, (n + 1) * WIDE)
                rows = pl.ds(pl.multiple_of(chip * 2 * WIDE, 2 * WIDE), 2 * WIDE)
                part = dot(RX[chip], WO[rows, cols])
                if g > 0:
                    part = part + PA[:, cols]
                if g < 3:
                    PA[:, cols] = part
                else:
                    for s in range(4):
                        some = slice(s * QUART, (s + 1) * QUART)
                        mine = G[own + s, :, cols].astype(F32)
                        out[some, cols] = (mine + MOD[2:3, cols] * part[some]).astype(BF16)

    with jax.named_scope("drain"):
        for slot in range(28):
            ag_copy(own, slot, to_mate).wait_send()

        @pl.loop(1, 16)
        def _(k):
            mp_copy(k).wait_send()

        for leg in range(4):
            for o in (1, 2, 3):
                cx_copy(leg, 0, o).wait_send()

        @pl.loop(1, 8)
        def _(k):
            ms_copy(tp, k).wait_send()

        for k in range(2, 7):
            aa_copy(tp, tp, k).wait_send()
        for i in range(2):
            relay_in(i).wait_send()
            relay_out(i).wait_send()

        for n in range(12):
            halo_copy(0, n).wait_send()


def shards(
    resid, cond, mod_shift, mod_scale, mod_gate, norm_gain, context, w_query, w_key, w_value,
    query_gain, key_gain, offset_bias, context_bias, w_out,
):
    vmem = pl.BlockSpec(memory_space=pltpu.VMEM)
    smem = pl.BlockSpec(memory_space=pltpu.SMEM)
    hbm = pl.BlockSpec(memory_space=pl.ANY)
    dma = pltpu.SemaphoreType.DMA
    scratch = [
        pltpu.VMEM((32, QUART, D), BF16),
        pltpu.VMEM((D, WIDE), BF16),
        pltpu.VMEM((D, WIDE), BF16),
        pltpu.VMEM((D, WIDE), BF16),
        pltpu.VMEM((D, D), BF16),
        pltpu.VMEM((64, D), BF16),
        pltpu.VMEM((SHARD, D), BF16),
        pltpu.VMEM((SHARD, 3 * WIDE), F32),
        pltpu.VMEM((TOK, WIDE), BF16),
        pltpu.VMEM((TOK + 2 * PAD, 2 * WIDE), BF16),
        pltpu.VMEM((CTX, WIDE), BF16),
        pltpu.VMEM((CTX, WIDE), BF16),
        pltpu.VMEM((16, 8, WIDE), F32),
        pltpu.VMEM((8, 8, WIDE), F32),
        pltpu.VMEM((8, WIDE), F32),
        pltpu.VMEM((8, D), F32),
        pltpu.VMEM((2, 16, 128), F32),
        pltpu.VMEM((2, 14, GRID_W, 128), F32),
        pltpu.VMEM((2, SHARD, CTX), F32),
        pltpu.VMEM((2, SHARD, CTX), BF16),
        pltpu.VMEM((2, SHARD, 512), F32),
        pltpu.VMEM((2, SHARD, 512), BF16),
        pltpu.VMEM((TOK + 2 * PAD, 3 * HEAD), BF16),
        pltpu.VMEM((CTX, 3 * HEAD), BF16),
        pltpu.VMEM((4, SHARD, WIDE), BF16),
        pltpu.VMEM((TOK, WIDE), F32),
        pltpu.VMEM((2, TOK, HEAD), F32),
        pltpu.VMEM((2, TOK, HEAD), F32),
        pltpu.VMEM((2, SHARD, HEAD), F32),
        pltpu.VMEM((SHARD, HEAD), F32),
        pltpu.VMEM((SHARD, D), F32),
        pltpu.VMEM((2, SHARD, WIDE), BF16),
        pltpu.VMEM((8, SHARD, WIDE), BF16),
        pltpu.VMEM((4, SHARD, 2 * WIDE), BF16),
        dma((9,)), dma((28,)), dma((32,)), dma((16,)), dma((16,)), dma((8,)), dma((8,)),
        dma((16,)), dma((16,)), dma((12,)), dma((12,)), dma((8,)), dma((8,)), dma((4,)), dma((2,)),
    ]
    return pl.pallas_call(
        kernel,
        out_shape=jax.ShapeDtypeStruct((SHARD, D), BF16),
        in_specs=[hbm, vmem, vmem, vmem, vmem, vmem, hbm, hbm, hbm, hbm, vmem, vmem, vmem, smem, hbm],
        out_specs=vmem,
        scratch_shapes=scratch,
        compiler_params=pltpu.CompilerParams(
            collective_id=0, has_side_effects=True, vmem_limit_bytes=60 * 1024 * 1024
        ),
    )(
        resid, cond.reshape(1, -1), mod_shift, mod_scale, mod_gate, norm_gain.reshape(1, -1),
        context, w_query, w_key, w_value, query_gain.reshape(1, -1), key_gain.reshape(1, -1),
        jnp.transpose(offset_bias, (1, 0, 2)), context_bias, w_out,
    )


def solution(mesh):
    grid = Mesh(mesh.devices.reshape(4, 4, 4, 2), ("z", "y", "x", "c"))
    sp, tp, both = ("z", "y"), ("x", "c"), ("z", "y", "x", "c")
    placed = (
        P(both, None), P(sp), P(sp, tp), P(sp, tp), P(sp, tp), P(), P(sp, None),
        P(None, tp), P(None, tp), P(None, tp), P(), P(), P(tp, None, None), P(tp), P(),
    )
    return jax.shard_map(
        shards, mesh=grid, in_specs=placed, out_specs=P(both, None), check_vma=False
    )
```

```python
import functools

import jax
import jax.numpy as jnp
from jax import lax
from jax.experimental import pallas as pl
from jax.experimental.pallas import tpu as pltpu
from jax.sharding import Mesh
from jax.sharding import PartitionSpec as P

MESH = pl.DeviceIdType.MESH
BF16, F32 = jnp.bfloat16, jnp.float32
EPS = 1e-06
LOG2E = 1.4426950408889634
HEAD = 128
GRID_W = 64
D = 2048
CTX = 1024
ROWS_DEV = 24
TOK = 1536
SHARD = 192
PAD = 288
HALF = 96
QUART = 48
WIDE = 256
NEG = -1e30
NT = (((1,), (1,)), ((), ()))


def dot_nt(a, b):
    return lax.dot_general(a, b, NT, preferred_element_type=F32)


def dot(a, b):
    return jnp.dot(a, b, preferred_element_type=F32)


def inv_rms(v):
    return lax.rsqrt(jnp.mean(v * v, axis=-1, keepdims=True) + EPS)


def kernel(
    resid, cond, mod_shift, mod_scale, mod_gate, norm_gain, context, w_query, w_key, w_value,
    query_gain, key_gain, offset_bias, context_bias, w_out, out,
    G, WQ, WK, WV, WO, CX, NRM, R, Q, KV, CK, CV, MP, MS, MSUM, MOD, OB, T2, S, PR, SW, PW, VA, CVA, QN, ACC, MC, LC, M, L, PA, RL, ATT, RX,
    load_sem, ag_send, ag_recv, mp_send, mp_recv, ms_send, ms_recv, cx_send, cx_recv,
    halo_send, halo_recv, aa_send, aa_recv, rl_send, rl_recv,
):
    z, y, x, c = (lax.axis_index(a) for a in ("z", "y", "x", "c"))
    sp, tp = z * 4 + y, x * 2 + c
    right, left, opp, mate = (x + 1) % 4, (x + 3) % 4, (x + 2) % 4, 1 - c

    def sp_dev(s):
        return (s // 4, s % 4, x, c)

    def tp_dev(t):
        return (z, y, t // 2, t % 2)

    with jax.named_scope("entry"):
        loads = [
            pltpu.make_async_copy(
                resid.at[pl.ds(n * QUART, QUART)], G.at[tp * 4 + n], load_sem.at[n]
            )
            for n in range(4)
        ] + [
            pltpu.make_async_copy(context, CX, load_sem.at[4]),
            pltpu.make_async_copy(w_key, WK, load_sem.at[5]),
            pltpu.make_async_copy(w_value, WV, load_sem.at[6]),
            pltpu.make_async_copy(w_query, WQ, load_sem.at[7]),
            pltpu.make_async_copy(w_out, WO, load_sem.at[8]),
        ]
        for one in loads:
            one.start()

        barrier = pltpu.get_barrier_semaphore()

        @pl.loop(1, 8)
        def _(k):
            pl.semaphore_signal(barrier, inc=1, device_id=tp_dev((tp + k) % 8), device_id_type=MESH)

        @pl.loop(1, 16)
        def _(k):
            pl.semaphore_signal(barrier, inc=1, device_id=sp_dev((sp + k) % 16), device_id_type=MESH)

        cf = cond[...].astype(F32)
        lifted = jnp.broadcast_to(cf / (1.0 + jnp.exp(-cf)), (16, 128)).astype(BF16)
        rows8 = lax.broadcasted_iota(jnp.int32, (8, WIDE), 0)
        p_shift = dot(lifted, mod_shift[...])[0:8]
        p_scale = dot(lifted, mod_scale[...])[0:8]
        p_gate = dot(lifted, mod_gate[...])[0:8]
        MP[sp] = jnp.where(rows8 == 0, p_shift, jnp.where(rows8 == 1, p_scale, p_gate))

        pl.semaphore_wait(barrier, 22)

    def ag_copy(chunk, slot, device):
        return pltpu.make_async_remote_copy(
            src_ref=G.at[chunk], dst_ref=G.at[chunk], send_sem=ag_send.at[slot],
            recv_sem=ag_recv.at[chunk], device_id=device, device_id_type=MESH,
        )

    to_right, to_left, to_mate = (z, y, right, c), (z, y, left, c), (z, y, x, mate)
    to_right, to_left, to_mate = (z, y, right, c), (z, y, left, c), (z, y, x, mate)
    own = tp * 4
    for n in range(4):
        loads[n].wait()
    ag_copy(own, 0, to_right).start()
    ag_copy(own + 3, 4, to_left).start()

    for n in range(4):
        ag_copy(own + n, 8 + n, to_mate).start()

    def mp_copy(k):
        return pltpu.make_async_remote_copy(
            src_ref=MP.at[sp], dst_ref=MP.at[sp], send_sem=mp_send.at[k],
            recv_sem=mp_recv.at[sp], device_id=sp_dev((sp + k) % 16), device_id_type=MESH,
        )

    def mp_wait(k):
        s = (sp + k) % 16
        return pltpu.make_async_remote_copy(
            src_ref=MP.at[s], dst_ref=MP.at[s], send_sem=mp_send.at[k],
            recv_sem=mp_recv.at[s], device_id=sp_dev(s), device_id_type=MESH,
        )

    @pl.loop(1, 16)
    def _(k):
        mp_copy(k).start()

    loads[4].wait()

    @pl.loop(0, 4)
    def _(i):
        rows = pl.ds(pl.multiple_of(i * 16, 16), 16)
        v = CX[rows, :].astype(F32)
        NRM[rows, :] = (v * inv_rms(v) * norm_gain[...]).astype(BF16)

    loads[5].wait()
    loads[6].wait()
    kg, qg = key_gain[...], query_gain[...]
    ck = dot(NRM[0:64, :], WK[...])
    cv = dot(NRM[0:64, :], WV[...])
    key_rows = pl.ds(pl.multiple_of(sp * 64, 64), 64)
    for h in range(2):
        part = ck[:, h * HEAD : (h + 1) * HEAD]
        CK[key_rows, h * HEAD : (h + 1) * HEAD] = (part * inv_rms(part) * kg).astype(BF16)
    CV[pl.ds(pl.multiple_of((y * 4 + z) * 64, 64), 64), :] = cv.astype(BF16)

    def cx_copy(leg, source, o):
        along_y = leg in (0, 3)
        ref, count = (CK, CV, CK, CV)[leg], 64 if leg < 2 else 256
        at = (source, source, source, source)[leg] * count + (0 if leg > 1 else (z, y)[leg] * 256)
        rows = pl.ds(pl.multiple_of(at, 64), count)
        return pltpu.make_async_remote_copy(
            src_ref=ref.at[rows], dst_ref=ref.at[rows], send_sem=cx_send.at[leg * 4 + o],
            recv_sem=cx_recv.at[leg * 4 + source],
            device_id=(z, (y + o) % 4, x, c) if along_y else ((z + o) % 4, y, x, c),
            device_id_type=MESH,
        )

    def cx_start(leg):
        for o in (2, 1, 3):
            cx_copy(leg, y if leg in (0, 3) else z, o).start()

    def cx_wait(leg):
        for o in (1, 3, 2):
            cx_copy(leg, ((y if leg in (0, 3) else z) + o) % 4, o).wait_recv()

    cx_start(0)
    cx_start(1)

    with jax.named_scope("mp_wait"):
        @pl.loop(1, 16)
        def _(k):
            mp_wait(k).wait_recv()

    total = MP[0]
    for s in range(1, 16):
        total = total + MP[s]
    MS[tp] = total

    def ms_copy(t, k):
        return pltpu.make_async_remote_copy(
            src_ref=MS.at[t], dst_ref=MS.at[t], send_sem=ms_send.at[k],
            recv_sem=ms_recv.at[t], device_id=tp_dev((tp + k) % 8), device_id_type=MESH,
        )

    @pl.loop(1, 8)
    def _(k):
        ms_copy(tp, k).start()

    for n in range(1, 4):
        ag_copy(own + n, n, to_right).start()
        ag_copy(own + 3 - n, 4 + n, to_left).start()

    with jax.named_scope("ctx_turn"):
        for leg in range(2):
            cx_wait(leg)
            cx_start(leg + 2)

    with jax.named_scope("bias"):
        OB[...] = jnp.zeros_like(OB)
        for h in range(2):
            OB[h, 0:15, 0:31] = offset_bias[:, h, :] * LOG2E
        col = lax.broadcasted_iota(jnp.int32, (GRID_W, 128), 0)
        lane = lax.broadcasted_iota(jnp.int32, (GRID_W, 128), 1)
        key_col = lane % GRID_W
        begin = jnp.clip(col - 8, 0, GRID_W - 16)
        valid = (key_col >= begin) & (key_col < begin + 16)
        for h in range(2):

            @pl.loop(0, 14)
            def _(o):
                one = jnp.broadcast_to(OB[h, pl.ds(o, 1), :], (GRID_W, 128))
                two = jnp.broadcast_to(OB[h, pl.ds(o + 1, 1), :], (GRID_W, 128))
                one = pltpu.roll(one, 113, 1, stride=1, stride_axis=0)
                two = pltpu.roll(two, 49, 1, stride=1, stride_axis=0)
                T2[h, o] = jnp.where(valid, jnp.where(lane < GRID_W, one, two), NEG)

    with jax.named_scope("ms_wait"):
        @pl.loop(1, 8)
        def _(k):
            ms_copy((tp + k) % 8, k).wait_recv()

    for t in range(8):
        cols = slice(t * WIDE, (t + 1) * WIDE)
        block = MS[t]
        MOD[0:1, cols] = block[0:1]
        MOD[1:2, cols] = norm_gain[:, cols] * (1.0 + block[1:2])
        MOD[2:3, cols] = block[2:3]

    loads[7].wait()

    lo = jnp.where(sp == 0, 0, -4)
    hi = jnp.where(sp == 15, 16, 20)
    factor = HEAD**-0.5 * LOG2E
    STRIPS = range(0, SHARD, 16)

    def piece_of(s, j):
        r, n, side = s // 2, s % 2, j % 2
        dx = jnp.where(r == 0, 0, jnp.where(r == 3, 2, 3 - 2 * side))
        core = c if j < 2 else mate
        shift = jnp.where(r == 2, 2, 0)
        later = n + shift if side == 0 else 3 - n - shift
        return (((x + dx) % 4) * 2 + core) * 4 + jnp.where(r == 0, 2 * n + side, later)

    def full(v):
        return jnp.broadcast_to(v, (16, 128))

    def tiles(v):
        return [v[:, n * 128 : (n + 1) * 128] for n in range(v.shape[1] // 128)]

    def tree(parts, op):
        while len(parts) > 1:
            parts = [op(p, q) for p, q in zip(parts[::2], parts[1::2])] + parts[len(parts) & ~1 :]
        return parts[0]

    def spread(ref, rows, new):
        ref[rows, 0:HEAD] = new[:, 0:HEAD]
        ref[rows, HEAD : 2 * HEAD] = jnp.ones_like(new[:, 0:HEAD])
        ref[rows, 2 * HEAD :] = new[:, HEAD:]

    def split(h, both):
        out_part, sums = both[:, 0:HEAD], both[:, HEAD:]
        return (out_part, sums) if h == 0 else (sums, out_part)

    def norm_rows(piece, at):
        for i in range(3):
            v = G[piece, i * 16 : i * 16 + 16, :].astype(F32)
            L[at + i * 16 : at + i * 16 + 16, :] = full(inv_rms(v))
        for i in range(3):
            rows = slice(at + i * 16, at + i * 16 + 16)
            inv = L[rows, :]
            for n in range(D // 128):
                cols = slice(n * 128, (n + 1) * 128)
                v = G[piece, i * 16 : i * 16 + 16, cols].astype(F32)
                NRM[rows, cols] = (v * inv * MOD[1:2, cols] + MOD[0:1, cols]).astype(BF16)

    def head_rows(piece, at, slot):
        for i in range(3):
            rows = slice(at + i * 16, at + i * 16 + 16)
            q_rows = pl.ds(pl.multiple_of(piece * QUART + i * 16, 16), 16)
            k_rows = pl.ds(pl.multiple_of(piece * QUART + i * 16 + PAD, 16), 16)
            for h in range(2):
                a, b = h * HEAD, (h + 1) * HEAD
                part = R[rows, a:b]
                part = (part * inv_rms(part) * qg).astype(BF16)
                Q[q_rows, a:b] = part
                QN[slot, rows, a:b] = part
                part = R[rows, WIDE + a : WIDE + b]
                KV[k_rows, a:b] = (part * inv_rms(part) * kg).astype(BF16)
            new = R[rows, 2 * WIDE :].astype(BF16)
            KV[k_rows, WIDE:] = new
            spread(VA, k_rows, new)

    def halo_copy(piece, k):
        src = pl.multiple_of(piece * QUART + PAD, 16)
        low = k < 6
        dst = pl.multiple_of(k * QUART + jnp.where(low, PAD + TOK, -PAD), 16)
        return pltpu.make_async_remote_copy(
            src_ref=KV.at[pl.ds(src, QUART)], dst_ref=KV.at[pl.ds(dst, QUART)],
            send_sem=halo_send.at[k], recv_sem=halo_recv.at[k],
            device_id=sp_dev((sp + jnp.where(low, 15, 1)) % 16), device_id_type=MESH,
        )

    def context_head(s, h, slot=None):
        slot = h if slot is None else slot
        pieces = [piece_of(s, j) for j in range(4)]
        a, b = h * HEAD, (h + 1) * HEAD
        cb = context_bias[h] * LOG2E

        def place(at):
            return pl.ds(pl.multiple_of(pieces[at // QUART] * QUART + at % QUART, 16), 16)

        S[slot] = dot_nt(QN[s % 4, :, a:b], CK[:, a:b])
        for at in STRIPS:
            top = tree(tiles(S[slot, at : at + 16, :]), jnp.maximum) * factor + cb
            MC[h, place(at), :] = full(jnp.max(top, axis=1, keepdims=True))
        for at in STRIPS:
            top = MC[h, place(at), :] - cb
            for n in range(CTX // 128):
                cols = slice(n * 128, (n + 1) * 128)
                PR[slot, at : at + 16, cols] = jnp.exp2(
                    S[slot, at : at + 16, cols] * factor - top
                ).astype(BF16)
        acc, sums = split(h, dot(PR[slot], CVA[:, a : a + WIDE]))
        for j in range(4):
            rows = pl.ds(pl.multiple_of(pieces[j] * QUART, 16), QUART)
            ACC[rows, a:b] = acc[j * QUART : (j + 1) * QUART]
            LC[h, rows, :] = sums[j * QUART : (j + 1) * QUART]

    def window_part(t, slot):
        base = pl.multiple_of(t * SHARD, SHARD)
        keys, offsets = [], []
        for i in range(3):
            row = t * 3 + i
            start = jnp.minimum(jnp.maximum(row - 4, lo), hi)
            keys.append(pl.ds(pl.multiple_of(start * GRID_W + PAD, 32), 512))
            offsets.append(start - row + 7)
        for h in range(2):
            a, b = h * HEAD, (h + 1) * HEAD
            for i in range(3):
                SW[slot + h, i * 64 : (i + 1) * 64, :] = dot_nt(
                    Q[pl.ds(base + i * 64, 64), a:b], KV[keys[i], a:b]
                )
        for h in range(2):
            a, b = h * HEAD, (h + 1) * HEAD

            for at in STRIPS:
                i, sub = at // 64, slice(at % 64, at % 64 + 16)
                scores = []
                for n in range(4):
                    cols = slice(n * 128, (n + 1) * 128)
                    scores.append(SW[slot + h, at : at + 16, cols] * factor + T2[h, offsets[i] + 2 * n, sub, :])
                    SW[slot + h, at : at + 16, cols] = scores[-1]
                top = jnp.max(tree(scores, jnp.maximum), axis=1, keepdims=True)
                M[slot + h, at : at + 16, :] = jnp.maximum(full(top), MC[h, pl.ds(base + at, 16), :])
            for at in STRIPS:
                top = M[slot + h, at : at + 16, :]
                for n in range(4):
                    cols = slice(n * 128, (n + 1) * 128)
                    PW[slot + h, at : at + 16, cols] = jnp.exp2(SW[slot + h, at : at + 16, cols] - top).astype(BF16)
            for i in range(3):
                part, rows = slice(i * 64, (i + 1) * 64), pl.ds(base + i * 64, 64)
                new, sums = split(h, dot(PW[slot + h, part, :], VA[keys[i], a : a + WIDE]))
                keep = jnp.exp2(MC[h, rows, :] - M[slot + h, part, :])
                norm = 1.0 / (sums + LC[h, rows, :] * keep)
                ATT[t, part, a:b] = ((new + ACC[rows, a:b] * keep) * norm).astype(BF16)

    def aa_copy(t, src, k):
        half = pl.ds(pl.multiple_of(src % 2 * WIDE, WIDE), WIDE)
        return pltpu.make_async_remote_copy(
            src_ref=ATT.at[t], dst_ref=RX.at[src // 2, :, half], send_sem=aa_send.at[k],
            recv_sem=aa_recv.at[src], device_id=tp_dev(t), device_id_type=MESH,
        )

    onward = jnp.where(c == 0, right, left)
    behind = jnp.where(c == 0, left, right)

    def relay_in(i):
        return pltpu.make_async_remote_copy(
            src_ref=ATT.at[opp * 2 + i], dst_ref=RL.at[i], send_sem=rl_send.at[i],
            recv_sem=rl_recv.at[i], device_id=(z, y, onward, c), device_id_type=MESH,
        )

    def relay_out(i):
        half = pl.ds(pl.multiple_of(c * WIDE, WIDE), WIDE)
        return pltpu.make_async_remote_copy(
            src_ref=RL.at[i], dst_ref=RX.at[behind, :, half], send_sem=rl_send.at[2 + i],
            recv_sem=aa_recv.at[behind * 2 + c], device_id=(z, y, onward, i), device_id_type=MESH,
        )

    first_low = jnp.where(tp == 1, 0, jnp.where(tp == 0, 1, 0))
    near = jnp.where(x < 2, 1, 3)

    def halo_wait(t):
        @pl.when(t == first_low)
        def _():
            with jax.named_scope("halo_low"):
                for n in range(6, 12):
                    halo_copy(n + 20, n).wait_recv()
            spread(VA, slice(0, PAD), KV[0:PAD, WIDE:])

        @pl.when(t == 7)
        def _():
            with jax.named_scope("halo_high"):
                for n in range(6):
                    halo_copy(n, n).wait_recv()
            spread(VA, slice(PAD + TOK, 2 * PAD + TOK), KV[PAD + TOK :, WIDE:])

    def mate_wait(s):
        with jax.named_scope("mate_wait"):
            for j in (2, 3):
                ag_copy(piece_of(s, j), 0, to_right).wait_recv()

    def norm_project(s, which):
        part = slice(which[0] * QUART, (which[-1] + 1) * QUART)
        for j in which:
            norm_rows(piece_of(s, j), j * QUART)
        for k, w in enumerate((WQ, WK, WV)):
            R[part, k * WIDE : (k + 1) * WIDE] = dot(NRM[part, :], w[...])

    def take_next(s):
        for j in range(2):
            piece = piece_of(s, j)
            with jax.named_scope("ring_wait"):
                ag_copy(piece, 0, to_right).wait_recv()
            ag_copy(piece, 8 + 2 * s + j, to_mate).start()

            @pl.when(s // 2 == 1)
            def _():
                ag_copy(piece, 24 + 2 * j + s % 2, to_right if j == 0 else to_left).start()

    def heads(s, which):
        for j in which:
            head_rows(piece_of(s, j), j * QUART, s % 4)

    def send_halo(s):
        for j in range(4):
            piece = piece_of(s, j)

            @pl.when((piece < 6) | (piece >= 26))
            def _():
                halo_copy(piece, jnp.where(piece < 6, piece, piece - 20)).start()

    ALL = (0, 1, 2, 3)

    @pl.loop(0, 3)
    def _(s):
        @pl.when(s > 0)
        def _():
            take_next(s + 1)

        mate_wait(s)
        with jax.named_scope("first_half"):
            norm_project(s, ALL)

        with jax.named_scope("second_half"):
            heads(s, ALL)
        send_halo(s)

    with jax.named_scope("ctx_wait"):
        cx_wait(2)
        cx_wait(3)

    for e in range(16):
        spread(CVA, slice(e * 64, e * 64 + 64), CV[pl.ds((e % 4 * 4 + e // 4) * 64, 64), :])
    with jax.named_scope("ctx01"):
        for e in range(2):
            for h in range(2):
                context_head(tp * 0 + e, h, 2 * e + h)

    s3, s7 = tp * 0 + 3, tp * 0 + 7
    mate_wait(s3)
    with jax.named_scope("project_s"):
        norm_project(s3, ALL)
        heads(s3, ALL)
    send_halo(s3)
    take_next(s3 + 1)
    with jax.named_scope("ctx23"):
        for e in range(2):
            for h in range(2):
                context_head(s3 - 1 + e, h, 2 * e + h)

    @pl.loop(4, 7)
    def _(s):
        mate_wait(s)
        with jax.named_scope("project_s"):
            norm_project(s, ALL)
            heads(s, ALL)
        send_halo(s)

        @pl.when(s < 6)
        def _():
            take_next(s + 1)

        with jax.named_scope("ctx_s"):
            context_head(s, 0)
            context_head(s, 1)

    take_next(s7)
    with jax.named_scope("last_own"):
        norm_project(s7, (0, 1))
        heads(s7, (0, 1))
    mate_wait(s7)
    with jax.named_scope("last_mate"):
        norm_project(s7, (2, 3))
        heads(s7, (2, 3))
    send_halo(s7)
    with jax.named_scope("ctx7"):
        context_head(7, 0)
        context_head(7, 1)

    middle = (x == 1) | (x == 2)

    with jax.named_scope("window"):
        @pl.loop(0, 8)
        def _(k):
            home = (k == 4) | (k == 5)
            side = jnp.where(middle, jnp.where(k < 4, near, 4 - near), 1 + k % 2 * 2)
            dx = jnp.where(home, 0, jnp.where(k < 2, 2, side))
            core = jnp.where(home, (mate + k) % 2, k % 2)
            core = jnp.where(middle | (k < 6) & (home | (k < 2)), core, k // 4)
            t = (x + dx) % 4 * 2 + core

            @pl.when((k == 5) | (k == 6))
            def _():
                with jax.named_scope("relay_wait"):
                    relay_in(k - 5).wait_recv()
                relay_out(k - 5).start()

            halo_wait(t)
            window_part(t, 0)

            @pl.when(k < 2)
            def _():
                relay_in(k).start()

            @pl.when((k >= 2) & (k != 5))
            def _():
                aa_copy(t, tp, k).start()

    own_half = pl.ds(pl.multiple_of(c * WIDE, WIDE), WIDE)
    RX[x, :, own_half] = ATT[tp]
    loads[8].wait()

    odd = x % 2
    for g, dx in enumerate((3 - 2 * odd, 0, 2, 1 + 2 * odd)):
        chip = (x + dx) % 4
        with jax.named_scope("aa_wait"):
            if g != 1:
                aa_copy(tp, chip * 2, 0).wait_recv()
                aa_copy(tp, chip * 2 + 1, 0).wait_recv()
            else:
                aa_copy(tp, x * 2 + mate, 0).wait_recv()
        with jax.named_scope("project"):
            for n in range(8):
                cols = slice(n * WIDE, (n + 1) * WIDE)
                rows = pl.ds(pl.multiple_of(chip * 2 * WIDE, 2 * WIDE), 2 * WIDE)
                part = dot(RX[chip], WO[rows, cols])
                if g > 0:
                    part = part + PA[:, cols]
                if g < 3:
                    PA[:, cols] = part
                else:
                    for s in range(4):
                        some = slice(s * QUART, (s + 1) * QUART)
                        mine = G[own + s, :, cols].astype(F32)
                        out[some, cols] = (mine + MOD[2:3, cols] * part[some]).astype(BF16)

    with jax.named_scope("drain"):
        for slot in range(28):
            ag_copy(own, slot, to_mate).wait_send()

        @pl.loop(1, 16)
        def _(k):
            mp_copy(k).wait_send()

        for leg in range(4):
            for o in (1, 2, 3):
                cx_copy(leg, 0, o).wait_send()

        @pl.loop(1, 8)
        def _(k):
            ms_copy(tp, k).wait_send()

        for k in (2, 3, 4, 6, 7):
            aa_copy(tp, tp, k).wait_send()
        for i in range(2):
            relay_in(i).wait_send()
            relay_out(i).wait_send()

        for n in range(12):
            halo_copy(0, n).wait_send()


def shards(
    resid, cond, mod_shift, mod_scale, mod_gate, norm_gain, context, w_query, w_key, w_value,
    query_gain, key_gain, offset_bias, context_bias, w_out,
):
    vmem = pl.BlockSpec(memory_space=pltpu.VMEM)
    smem = pl.BlockSpec(memory_space=pltpu.SMEM)
    hbm = pl.BlockSpec(memory_space=pl.ANY)
    dma = pltpu.SemaphoreType.DMA
    scratch = [
        pltpu.VMEM((32, QUART, D), BF16),
        pltpu.VMEM((D, WIDE), BF16),
        pltpu.VMEM((D, WIDE), BF16),
        pltpu.VMEM((D, WIDE), BF16),
        pltpu.VMEM((D, D), BF16),
        pltpu.VMEM((64, D), BF16),
        pltpu.VMEM((SHARD, D), BF16),
        pltpu.VMEM((SHARD, 3 * WIDE), F32),
        pltpu.VMEM((TOK, WIDE), BF16),
        pltpu.VMEM((TOK + 2 * PAD, 2 * WIDE), BF16),
        pltpu.VMEM((CTX, WIDE), BF16),
        pltpu.VMEM((CTX, WIDE), BF16),
        pltpu.VMEM((16, 8, WIDE), F32),
        pltpu.VMEM((8, 8, WIDE), F32),
        pltpu.VMEM((8, WIDE), F32),
        pltpu.VMEM((8, D), F32),
        pltpu.VMEM((2, 16, 128), F32),
        pltpu.VMEM((2, 14, GRID_W, 128), F32),
        pltpu.VMEM((4, SHARD, CTX), F32),
        pltpu.VMEM((4, SHARD, CTX), BF16),
        pltpu.VMEM((4, SHARD, 512), F32),
        pltpu.VMEM((4, SHARD, 512), BF16),
        pltpu.VMEM((TOK + 2 * PAD, 3 * HEAD), BF16),
        pltpu.VMEM((CTX, 3 * HEAD), BF16),
        pltpu.VMEM((4, SHARD, WIDE), BF16),
        pltpu.VMEM((TOK, WIDE), F32),
        pltpu.VMEM((2, TOK, HEAD), F32),
        pltpu.VMEM((2, TOK, HEAD), F32),
        pltpu.VMEM((4, SHARD, HEAD), F32),
        pltpu.VMEM((SHARD, HEAD), F32),
        pltpu.VMEM((SHARD, D), F32),
        pltpu.VMEM((2, SHARD, WIDE), BF16),
        pltpu.VMEM((8, SHARD, WIDE), BF16),
        pltpu.VMEM((4, SHARD, 2 * WIDE), BF16),
        dma((9,)), dma((28,)), dma((32,)), dma((16,)), dma((16,)), dma((8,)), dma((8,)),
        dma((16,)), dma((16,)), dma((12,)), dma((12,)), dma((8,)), dma((8,)), dma((4,)), dma((2,)),
    ]
    return pl.pallas_call(
        kernel,
        out_shape=pltpu.VMEM((SHARD, D), BF16),
        in_specs=[hbm, vmem, vmem, vmem, vmem, vmem, hbm, hbm, hbm, hbm, vmem, vmem, vmem, smem, hbm],
        out_specs=vmem,
        scratch_shapes=scratch,
        compiler_params=pltpu.CompilerParams(
            collective_id=0, has_side_effects=True, vmem_limit_bytes=60 * 1024 * 1024
        ),
    )(
        resid, cond.reshape(1, -1), mod_shift, mod_scale, mod_gate, norm_gain.reshape(1, -1),
        context, w_query, w_key, w_value, query_gain.reshape(1, -1), key_gain.reshape(1, -1),
        jnp.transpose(offset_bias, (1, 0, 2)), context_bias, w_out,
    )


def solution(mesh):
    grid = Mesh(mesh.devices.reshape(4, 4, 4, 2), ("z", "y", "x", "c"))
    sp, tp, both = ("z", "y"), ("x", "c"), ("z", "y", "x", "c")
    placed = (
        P(both, None), P(sp), P(sp, tp), P(sp, tp), P(sp, tp), P(), P(sp, None),
        P(None, tp), P(None, tp), P(None, tp), P(), P(), P(tp, None, None), P(tp), P(),
    )
    return jax.shard_map(
        shards, mesh=grid, in_specs=placed, out_specs=P(both, None), check_vma=False
    )
```
